32 devices in a mesh: sp: 8 (over z, x), tp: 4 (over y, core).
Axes of the slice: x: 2, y: 2, z: 4, core: 2. Of those that a mesh axis runs over, the one named last changes fastest.
Arguments:
- inputs: bfloat16 [4096, 2048], P('sp', 'tp'), may hold values from -45 to 45
- norm_gain: float32 [3, 2048], replicated, may hold values from 0.1 to 1.9
- w_value: bfloat16 [3, 2048, 1024], P(None, 'sp', 'tp'), may hold values from -0.125 to 0.125
- w_gate: bfloat16 [3, 2048, 1024], P(None, 'sp', 'tp'), may hold values from -0.125 to 0.125
- conv_taps: float32 [3, 31, 1024], P(None, None, 'tp'), may hold values from -5 to 5
- ln_gain: float32 [3, 1024], P(None, 'tp'), may hold values from 0.1 to 1.9
- ln_bias: float32 [3, 1024], P(None, 'tp'), may hold values from -3 to 3
- w_out: bfloat16 [3, 1024, 2048], P(None, 'tp', 'sp'), may hold values from -0.1875 to 0.1875
Outputs:
- stream: bfloat16 [4096, 2048], P('sp', 'tp')
The draws below stay inside these ranges and needn't reach their ends.
All inputs are finite; a program needn't handle non-finite values.
Results may differ from the reference program's by a relative error of at most 0.01.
Values may be sent and summed in bfloat16 or wider, within the bound.
A program may use at most 64 MiB of HBM per device.

```python
import jax
import jax.numpy as jnp
from jax import lax

D = 2048
C = 1024
K = 31
LAYERS = 3
TOKENS = 4096
N_TP = 4


def draw_inputs(key, part):
    key_a, key_b = jax.random.split(jax.random.fold_in(key, 11), 2)
    ramp = 10.0 ** (0.5 * jnp.arange(D, dtype=jnp.float32) / D + 0.3 * jax.random.uniform(key_b, (D,), jnp.float32))
    base = jnp.clip(jax.random.normal(key_a, (TOKENS, D), jnp.float32), -4.0, 4.0)
    return (base * ramp[None, :]).astype(jnp.bfloat16)


def draw_conv_taps(key, part):
    key_a, key_b = jax.random.split(jax.random.fold_in(key, 23), 2)
    ramp = K ** (-0.5) * 10.0 ** (0.5 * jnp.arange(C, dtype=jnp.float32) / C + 0.3 * jax.random.uniform(key_b, (LAYERS, 1, C), jnp.float32))
    base = jnp.clip(jax.random.normal(key_a, (LAYERS, K, C), jnp.float32), -4.0, 4.0)
    return base * ramp


def levels(key, shape, cuts, low, high):
    factor_of = 1.0
    for dim, blocks in cuts:
        draws = jax.random.uniform(jax.random.fold_in(jax.random.fold_in(key, 6), dim), (blocks,), jnp.float32, low / len(cuts), high / len(cuts))
        factor_of = factor_of * jnp.repeat(jnp.exp(draws), shape[dim] // blocks).reshape((-1,) + (1,) * (len(shape) - 1 - dim))
    return factor_of


def normal_values(stream_key, shape, width, bound, cuts=(), kind=jnp.bfloat16):
    loudness = levels(stream_key, shape, cuts, -0.22, 0.18) if cuts else 1.0
    values = jax.random.normal(stream_key, shape, jnp.float32) * width * loudness
    return jnp.minimum(jnp.maximum(values, -bound), bound).astype(kind)


def setup_inputs(seed: int = 0) -> dict:
    streams_of = jax.random.split(jax.random.key(seed), 9)
    inputs = draw_inputs(jax.random.fold_in(streams_of[8], 71), 0)
    norm_gain = jnp.clip(1.0 + 0.18 * jax.random.normal(streams_of[1], (LAYERS, D), jnp.float32), 0.1, 1.9)
    w_value = normal_values(streams_of[2], (LAYERS, D, C), D ** -0.5, 0.125, ((1, 8), (2, 4)))
    w_gate = normal_values(streams_of[3], (LAYERS, D, C), D ** -0.5, 0.125, ((1, 8), (2, 4)))
    conv_taps = draw_conv_taps(jax.random.fold_in(streams_of[8], 71), 0)
    ln_gain = jnp.clip(1.0 + 0.18 * jax.random.normal(streams_of[5], (LAYERS, C), jnp.float32), 0.1, 1.9)
    ln_bias = normal_values(streams_of[6], (LAYERS, C), 0.5, 3.0, ((1, 4),), jnp.float32)
    w_out = normal_values(streams_of[7], (LAYERS, C, D), C ** -0.5, 0.1875, ((1, 4), (2, 8)))
    return {"inputs": inputs, "norm_gain": norm_gain, "w_value": w_value, "w_gate": w_gate, "conv_taps": conv_taps, "ln_gain": ln_gain, "ln_bias": ln_bias, "w_out": w_out}


def reference(inputs, norm_gain, w_value, w_gate, conv_taps, ln_gain, ln_bias, w_out):
    block = C // N_TP
    stream = inputs
    for layer in range(LAYERS):
        xf = stream.astype(jnp.float32)
        meansq = lax.optimization_barrier(jnp.mean(xf * xf, axis=1, keepdims=True))
        hidden = (xf * lax.rsqrt(meansq + 1e-06) * norm_gain[layer][None, :]).astype(jnp.bfloat16)
        value = jnp.dot(hidden, w_value[layer], preferred_element_type=jnp.float32)
        gate = jnp.dot(hidden, w_gate[layer], preferred_element_type=jnp.float32)
        glu = (value * jax.nn.sigmoid(gate)).astype(jnp.bfloat16)
        padded = jnp.pad(glu.astype(jnp.float32), ((K - 1, 0), (0, 0)))
        filtered = jnp.zeros((TOKENS, C), jnp.float32)
        for tap in range(K):
            filtered = filtered + conv_taps[layer, tap][None, :] * padded[tap:tap + TOKENS]
        mean_val = lax.optimization_barrier(jnp.mean(filtered, axis=1, keepdims=True))
        var_val = lax.optimization_barrier(jnp.mean(filtered * filtered, axis=1, keepdims=True)) - mean_val * mean_val
        normed = jax.nn.silu((filtered - mean_val) * lax.rsqrt(var_val + 1e-06) * ln_gain[layer][None, :] + ln_bias[layer][None, :]).astype(jnp.bfloat16)
        branch = jnp.zeros((TOKENS, D), jnp.float32)
        for part_index in range(N_TP):
            piece = jnp.dot(normed[:, part_index * block:(part_index + 1) * block], w_out[layer, part_index * block:(part_index + 1) * block], preferred_element_type=jnp.float32).astype(jnp.bfloat16)
            branch = branch + piece.astype(jnp.float32)
        stream = (xf + branch).astype(jnp.bfloat16)
    return stream
```

```python
import functools

import jax
import jax.numpy as jnp
from jax import lax
from jax.experimental import pallas as pl
from jax.experimental.pallas import tpu as pltpu
from jax.sharding import PartitionSpec as P

MESH = pl.DeviceIdType.MESH
PAIR = 2
CHUNK = 128
HALO = 32
LANES = 128
V, G, O, UP, OVER, ZOWN, XOWN = 0, 1, 2, 3, 4, 5, 6
OWN_X = ((XOWN, V, 1), (XOWN, G, 1))
OWN_Z = ((ZOWN, V, 1), (ZOWN, G, 1))


def every(kind, later):
    return tuple((kind, j, later) for j in range(4))


END_OPEN = (
    (V, 0, 0), *OWN_Z, (G, 0, 0), (V, 1, 0), (G, 1, 0), (V, 2, 0), (G, 2, 0), *OWN_X, (O, 0, 0),
)
HEAD_OPEN = (
    (V, 0, 0), *every(UP, 0), *OWN_Z, (G, 0, 0), (V, 1, 0), (G, 1, 0), (V, 2, 0), (G, 2, 0), *OWN_X, *every(OVER, 0),
)
MID_OPEN = (
    (V, 0, 0), (V, 1, 0), (G, 0, 0), (G, 1, 0), (V, 2, 0), (G, 2, 0), *OWN_X, (ZOWN, V, 1), *every(O, 0), (ZOWN, G, 1),
)
NEXT_OPEN = MID_OPEN
END_PLAN = {
    1: ((O, 1, 0),), 2: ((O, 2, 0),), 3: ((O, 3, 0),), 4: ((V, 0, 1),), 5: ((V, 1, 1), (ZOWN, V, 2), (ZOWN, G, 2)),
    6: ((V, 2, 1),), 7: ((G, 0, 1),), 8: ((G, 1, 1),), 9: ((G, 2, 1), (XOWN, V, 2), (XOWN, G, 2)), 12: ((O, 0, 1),),
}
HEAD_PLAN = {
    3: every(UP, 1), 4: ((V, 0, 1),), 5: ((V, 1, 1), (ZOWN, V, 2), (ZOWN, G, 2)), 6: ((V, 2, 1),),
    7: ((G, 0, 1),), 8: ((G, 1, 1),), 9: ((G, 2, 1), (XOWN, V, 2), (XOWN, G, 2), *every(OVER, 1)),
}
MID_PLAN = {
    1: ((V, 0, 1),), 2: ((V, 1, 1),), 3: ((V, 2, 1),), 4: ((G, 0, 1),), 5: ((G, 1, 1),),
    6: ((G, 2, 1), (XOWN, V, 2), (XOWN, G, 2), (ZOWN, V, 2)),
    9: ((O, 0, 1),), 10: ((O, 1, 1),), 11: ((O, 2, 1),), 12: ((O, 3, 1), (ZOWN, G, 2)),
}
NEXT_PLAN = {
    1: ((V, 0, 1),), 2: ((V, 1, 1),), 3: ((V, 2, 1),), 4: ((G, 0, 1), (UP, 0, 1)), 5: ((G, 1, 1), (UP, 1, 1)),
    6: ((G, 2, 1), (UP, 2, 1), (XOWN, V, 2), (XOWN, G, 2), (ZOWN, V, 2)), 7: ((UP, 3, 1),),
    8: (*every(OVER, 1), (ZOWN, G, 2)),
}


def fused_kernel(
    n_sp, n_tp, eps,
    x_ref, gain_ref, wv_ref, wg_ref, taps_ref, lng_ref, lnb_ref, wo_ref,
    out_ref,
    wv_all, wg_all, wo_all, xf, hid, glu, filt, rim_out, rim_in, stat, nrm,
    w_recv, w_zsend, w_xsend, o_recv, o_send, og_send,
    ag_recv, ag_send, rim_s, rim_r, st_recv, st_send, nr_recv, nr_send,
):
    sp = lax.axis_index("sp")
    tp = lax.axis_index("tp")
    layers, depth = wv_ref.shape[0], wv_ref.shape[1]
    rows, dblk = x_ref.shape
    width = wo_ref.shape[2]
    chan = wv_ref.shape[2]
    taps = taps_ref.shape[1]
    features = dblk * n_tp
    channels = chan * n_tp
    n_chunks = rows // CHUNK
    n_out = n_sp // PAIR
    outer, inner = lax.div(sp, PAIR), lax.rem(sp, PAIR)
    x_peer = outer * PAIR + (PAIR - 1 - inner)
    far_half, core = lax.div(tp, PAIR), lax.rem(tp, PAIR)
    partner = far_half * PAIR + (PAIR - 1 - core)
    far = (n_tp // PAIR - 1 - far_half) * PAIR + core
    first_off = HALO - (taps - 1)
    halves = chan // LANES

    last = n_out - 1
    upper = lax.div(outer, n_out // 2)
    near_end = outer + upper * (last - 2 * outer)

    def line(j):
        near = j + 1 - (near_end if j == 0 else 0)
        return near + upper * (last - 2 * near)

    slant = sp + 2 * inner - 1
    has_slant = (slant >= 0) & (slant < n_sp)
    barrier = pltpu.get_barrier_semaphore()

    def greet(sp_to, tp_to):
        pl.semaphore_signal(barrier, inc=1, device_id=(sp_to, tp_to), device_id_type=MESH)

    greet(line(0) * PAIR + inner, tp)
    greet(x_peer, tp)
    for step in range(1, n_tp):
        greet(sp, lax.rem(tp + step, n_tp))

    @pl.when(near_end == 1)
    def _():
        greet(line(1) * PAIR + inner, tp)

    @pl.when(has_slant)
    def _():
        greet(slant, tp)

    xf[tp] = x_ref[...]

    def own_rows(s):
        return pl.ds(pl.multiple_of(s * depth, depth), depth)

    def o_slot(l, x, b):
        return wo_all.at[l, x, pl.ds(pl.multiple_of(b * chan, chan), chan), :]

    def own_weights(l, carry):
        wv_all[l, own_rows(sp), :] = wv_ref[l]
        wg_all[l, own_rows(sp), :] = wg_ref[l]

        @pl.when(outer == tp)
        def _():
            wo_all[l, inner, pl.ds(pl.multiple_of(tp * chan, chan), chan), :] = wo_ref[l]

        return carry

    lax.fori_loop(0, layers, own_weights, 0)
    pl.semaphore_wait(barrier, 2 + n_tp - 1 + near_end + has_slant.astype(jnp.int32))

    def chunk_rows(c):
        return pl.ds(pl.multiple_of(c * CHUNK, CHUNK), CHUNK)

    def remote(src, dst, send, recv, sp_to, tp_to):
        return pltpu.make_async_remote_copy(
            src_ref=src, dst_ref=dst, send_sem=send, recv_sem=recv,
            device_id=(sp_to, tp_to), device_id_type=MESH,
        )

    w_in = (wv_ref, wg_ref)

    def w_slot(m, l, s):
        return (wv_all, wg_all)[m].at[l, own_rows(s), :]

    def z_copy(m, l, j):
        to = line(j) * PAIR + inner
        return remote(w_in[m].at[l], w_slot(m, l, sp), w_zsend.at[l, m, j], w_recv.at[l, m, sp], to, tp)

    def z_arrival(m, l, j):
        s = line(j) * PAIR + inner
        return remote(w_in[m].at[l], w_slot(m, l, s), w_zsend.at[l, m, j], w_recv.at[l, m, s], s, tp)

    def z_forward(m, l, j):
        s = line(j) * PAIR + inner
        to = line(1 if j == 0 else 0) * PAIR + inner
        slot = w_slot(m, l, s)
        return remote(slot, slot, w_zsend.at[l, m, PAIR + j], w_recv.at[l, m, s], to, tp)

    def x_own(m, l):
        return remote(w_in[m].at[l], w_slot(m, l, sp), w_xsend.at[l, m, last], w_recv.at[l, m, sp], x_peer, tp)

    def x_copy(m, l, j):
        s = line(j) * PAIR + inner
        slot = w_slot(m, l, s)
        return remote(slot, slot, w_xsend.at[l, m, j], w_recv.at[l, m, s], x_peer, tp)

    def x_arrival(m, l, z):
        s = z * PAIR + (PAIR - 1 - inner)
        slot = w_slot(m, l, s)
        return remote(slot, slot, w_xsend.at[l, m, last], w_recv.at[l, m, s], x_peer, tp)

    def side_copy(m, l):
        to = line(0) * PAIR + inner
        slot = w_slot(m, l, x_peer)
        return remote(slot, slot, w_xsend.at[l, m, 0], w_recv.at[l, m, x_peer], to, tp)

    def z_own(m, l):
        z_copy(m, l, 0).start()

        @pl.when(near_end == 1)
        def _():
            z_copy(m, l, 1).start()

    def relay_piece(m, l, j, side):
        z_arrival(m, l, j).wait_recv()

        @pl.when(near_end == 1)
        def _():
            z_forward(m, l, j).start()

        if j == 0 and side:
            x_arrival(m, l, outer).wait_recv()
            side_copy(m, l).start()
        else:
            x_copy(m, l, j).start()

    def w_ready(m, l):
        if m == 1:
            @pl.when(l == 0)
            def _():
                x_arrival(m, l, outer).wait_recv()
        else:
            x_arrival(m, l, outer).wait_recv()
        for j in range(last):
            x_arrival(m, l, line(j)).wait_recv()

    def o_gather(l):
        return remote(wo_ref.at[l], o_slot(l, inner, tp), og_send.at[l], o_recv.at[l, tp, inner], sp, outer)

    def o_hop(l, j, way, to):
        b = lax.rem(tp + j, n_tp)
        slot = o_slot(l, inner, b)
        return remote(slot, slot, o_send.at[l, j, way], o_recv.at[l, b, inner], to, tp)

    def o_arrival(l, b, x):
        slot = o_slot(l, x, b)
        return remote(slot, slot, o_send.at[l, 0, 0], o_recv.at[l, b, x], x_peer, tp)

    goes_up = (outer >= tp) & (outer < last)
    goes_down = (outer <= tp) & (outer > 0)

    def send_o(l):
        @pl.when(outer != tp)
        def _():
            o_gather(l).start()

    def o_arrived(l, j):
        if j == 0:
            @pl.when(outer != tp)
            def _():
                o_arrival(l, tp, inner).wait_recv()
        else:
            o_arrival(l, lax.rem(tp + j, n_tp), inner).wait_recv()

    def o_along(l, j):
        @pl.when(goes_up)
        def _():
            o_hop(l, j, 0, sp + PAIR).start()

        @pl.when(goes_down)
        def _():
            o_hop(l, j, 1, sp - PAIR).start()

    def relay_o(l, j, kind):
        if kind != OVER:
            o_arrived(l, j)
            o_along(l, j)
        if kind != UP:
            o_hop(l, j, 2, x_peer).start()

    def o_ready(l):
        for j in range(n_tp):
            o_arrival(l, lax.rem(tp + j, n_tp), PAIR - 1 - inner).wait_recv()

    def ag_far(c):
        r = chunk_rows(c)
        return remote(xf.at[tp, r, :], xf.at[tp, r, :], ag_send.at[0, c], ag_recv.at[0, c], sp, far)

    def ag_partner(c):
        r = chunk_rows(c)
        return remote(xf.at[tp, r, :], xf.at[tp, r, :], ag_send.at[1, c], ag_recv.at[1, c], sp, partner)

    def ag_forward(c):
        r = chunk_rows(c)
        return remote(xf.at[far, r, :], xf.at[far, r, :], ag_send.at[2, c], ag_recv.at[2, c], sp, partner)

    def nr_far(c):
        r = chunk_rows(c)
        return remote(nrm.at[tp, r, :], nrm.at[tp, r, :], nr_send.at[0, c], nr_recv.at[0, c], sp, far)

    def nr_partner(c):
        r = chunk_rows(c)
        return remote(nrm.at[tp, r, :], nrm.at[tp, r, :], nr_send.at[1, c], nr_recv.at[1, c], sp, partner)

    def nr_forward(c):
        r = chunk_rows(c)
        return remote(nrm.at[far, r, :], nrm.at[far, r, :], nr_send.at[2, c], nr_recv.at[2, c], sp, partner)

    def stat_copy(l, c, step):
        to = lax.rem(tp + step, n_tp)
        return remote(stat.at[l, c, tp], stat.at[l, c, tp], st_send.at[c, step], st_recv.at[c, tp], sp, to)

    def stat_arrival(l, c, step):
        src = lax.rem(tp + step, n_tp)
        return remote(stat.at[l, c, src], stat.at[l, c, src], st_send.at[c, step], st_recv.at[c, src], sp, src)

    def rim_copy(l):
        to = lax.rem(sp + 1, n_sp)
        return remote(rim_out.at[l], rim_in.at[l], rim_s.at[l], rim_r.at[l], to, tp)

    def do_pass(c):
        ag_far(c).wait_recv()
        ag_forward(c).start()

    def do_glu(l, c):
        ag_partner(c).wait_recv()
        ag_forward(c).wait_recv()
        r = chunk_rows(c)
        blocks = [xf[b, r, :].astype(jnp.float32) for b in range(n_tp)]
        total = sum(jnp.sum(b * b, axis=1, keepdims=True) for b in blocks)
        scale = lax.rsqrt(total / features + eps)
        for b in range(n_tp):
            cols = slice(b * dblk, (b + 1) * dblk)
            hid[:, cols] = (xf[b, r, :].astype(jnp.float32) * scale * gain_ref[pl.ds(l, 1), cols]).astype(jnp.bfloat16)
        h = hid[...]
        value = jnp.dot(h, wv_all[l], preferred_element_type=jnp.float32)
        gate = jnp.dot(h, wg_all[l], preferred_element_type=jnp.float32)
        g = (value * jax.nn.sigmoid(gate)).astype(jnp.bfloat16)
        for k in range(halves):
            glu[k, pl.ds(pl.multiple_of(HALO + c * CHUNK, HALO), CHUNK), :] = g[:, k * LANES:(k + 1) * LANES].astype(jnp.float32)

        @pl.when((c == n_chunks - 1) & (sp < n_sp - 1))
        def _():
            rim_out[l] = g[CHUNK - HALO:, :]
            rim_copy(l).start()

    def do_conv(l, c):
        @pl.when((c == 0) & (sp > 0))
        def _():
            rim_copy(l).wait_recv()
            rim = rim_in[l].astype(jnp.float32)
            for k in range(halves):
                glu[k, 0:HALO, :] = rim[:, k * LANES:(k + 1) * LANES]

        @pl.when((c == 0) & (sp == 0))
        def _():
            glu[:, 0:HALO, :] = jnp.zeros((halves, HALO, LANES), jnp.float32)

        r = chunk_rows(c)
        sums = jnp.zeros((CHUNK, 1), jnp.float32)
        squares = jnp.zeros((CHUNK, 1), jnp.float32)
        for k in range(halves):
            acc = jnp.zeros((CHUNK, LANES), jnp.float32)
            for tap in range(taps):
                acc = acc + taps_ref[l, tap:tap + 1, k * LANES:(k + 1) * LANES] * glu[
                    k, pl.ds(c * CHUNK + first_off + tap, CHUNK), :]
            filt[r, k * LANES:(k + 1) * LANES] = acc
            sums = sums + jnp.sum(acc, axis=1, keepdims=True)
            squares = squares + jnp.sum(acc * acc, axis=1, keepdims=True)
        lane = lax.broadcasted_iota(jnp.int32, (CHUNK, LANES), 1)
        both = jnp.where(lane == 0, sums, squares)
        stat[l, c, tp] = jnp.transpose(both)[0:8, :]
        for step in range(1, n_tp):
            stat_copy(l, c, step).start()

    def do_norm(l, c):
        for step in range(1, n_tp):
            stat_arrival(l, c, step).wait_recv()
        r = chunk_rows(c)
        tot = stat[l, c, 0]
        for b in range(1, n_tp):
            tot = tot + stat[l, c, b]
        tot = jnp.transpose(jnp.concatenate([tot, jnp.zeros((LANES - 8, CHUNK), jnp.float32)], axis=0))
        mean = tot[:, 0:1] / channels
        var = tot[:, 1:2] / channels - mean * mean
        pre = (filt[r, :] - mean) * lax.rsqrt(var + eps) * lng_ref[pl.ds(l, 1), :] + lnb_ref[pl.ds(l, 1), :]
        nrm[tp, r, :] = jax.nn.silu(pre).astype(jnp.bfloat16)
        ag_far(c).wait_send()
        ag_partner(c).wait_send()
        ag_forward(c).wait_send()
        for step in range(1, n_tp):
            stat_copy(l, c, step).wait_send()
        nr_far(c).start()
        nr_partner(c).start()

    def do_hand(c):
        nr_far(c).wait_recv()
        nr_forward(c).start()

    def do_out(l, c):
        nr_partner(c).wait_recv()
        nr_forward(c).wait_recv()
        r = chunk_rows(c)
        full = jnp.concatenate([nrm[b, r, :] for b in range(n_tp)], axis=1)
        for q in range(PAIR):
            cols = slice(q * width, (q + 1) * width)
            branch = jnp.dot(full, wo_all[l, q], preferred_element_type=jnp.float32)
            out_ref[r, cols] = (xf[tp, r, cols].astype(jnp.float32) + branch).astype(jnp.bfloat16)

        nr_far(c).wait_send()
        nr_partner(c).wait_send()
        nr_forward(c).wait_send()

        @pl.when(l < layers - 1)
        def _():
            xf[tp, r, :] = out_ref[r, :]
            ag_far(c).start()
            ag_partner(c).start()

    by_head = near_end * (outer - tp) * (outer - tp) * (1 - (far_half - core) * (far_half - core)) == 1
    is_mid = (near_end == 1) & jnp.logical_not(by_head)
    is_head = (near_end == 0) & (outer == tp)
    is_end = (near_end == 0) & (outer != tp)

    roles = (
        (is_end, END_OPEN, END_PLAN), (is_head, HEAD_OPEN, HEAD_PLAN),
        (is_mid, MID_OPEN, MID_PLAN), (by_head, NEXT_OPEN, NEXT_PLAN),
    )

    def act(kind, j, l, side):
        if kind == ZOWN:
            z_own(j, l)
        elif kind == XOWN:
            x_own(j, l).start()
        elif kind >= O:
            relay_o(l, j, kind)
        else:
            relay_piece(kind, l, j, side and kind == G)

    for m in (V, G):
        z_own(m, 0)
        x_own(m, 0).start()
    send_o(0)
    for c in range(n_chunks):
        ag_far(c).start()
        ag_partner(c).start()
    for role, order, _ in roles:
        @pl.when(role)
        def _():
            for kind, j, later in order:
                act(kind, j, later, False)

    for c in range(n_chunks):
        do_pass(c)
    w_ready(V, 0)
    w_ready(G, 0)

    def layer_body(l, carry):
        more = l < layers - 1

        def at(k):
            return lax.rem(l + k, n_chunks)

        def ahead(f):
            pl.when(more)(f)

        def slot(n):
            for role, _, plan in roles:
                for kind, j, later in plan.get(n, ()):
                    @pl.when((role & (l + later < layers)) if later else role)
                    def _():
                        act(kind, j, l + later, True)

        def pass_next(k):
            ahead(lambda: do_pass(at(k + 1)))

        do_glu(l, at(0))
        do_glu(l, at(1))
        do_conv(l, at(1))
        ahead(lambda: send_o(l + 1))
        slot(1)
        do_glu(l, at(2))
        do_conv(l, at(2))
        do_glu(l, at(3))
        slot(2)
        do_conv(l, at(3))
        do_norm(l, at(1))
        do_conv(l, at(0))
        do_norm(l, at(2))
        do_norm(l, at(3))
        slot(3)
        do_norm(l, at(0))
        slot(4)
        do_hand(at(1))
        do_hand(at(2))
        slot(5)
        do_hand(at(3))
        do_hand(at(0))
        slot(6)
        o_ready(l)
        do_out(l, at(1))
        do_out(l, at(2))
        slot(7)
        do_out(l, at(3))
        do_out(l, at(0))

        slot(8)
        pass_next(0)
        slot(9)
        pass_next(1)
        slot(10)
        pass_next(2)
        slot(11)
        pass_next(3)
        slot(12)

        @pl.when(more)
        def _():
            w_ready(V, l + 1)
            w_ready(G, l + 1)

        return carry

    lax.fori_loop(0, layers, layer_body, 0)

    def drain(l, carry):
        for m in range(PAIR):
            z_copy(m, l, 0).wait_send()

            @pl.when(near_end == 1)
            def _():
                z_copy(m, l, 1).wait_send()
                for j in range(last):
                    z_forward(m, l, j).wait_send()

            for j in range(last):
                x_copy(m, l, j).wait_send()
            x_own(m, l).wait_send()

        @pl.when(outer != tp)
        def _():
            o_gather(l).wait_send()

        for j in range(n_tp):
            @pl.when(goes_up)
            def _():
                o_hop(l, j, 0, sp + PAIR).wait_send()

            @pl.when(goes_down)
            def _():
                o_hop(l, j, 1, sp - PAIR).wait_send()

            o_hop(l, j, 2, x_peer).wait_send()

        @pl.when(sp < n_sp - 1)
        def _():
            rim_copy(l).wait_send()

        return carry

    lax.fori_loop(0, layers, drain, 0)


def fused_shards(n_sp, n_tp, inputs, norm_gain, w_value, w_gate, conv_taps, ln_gain, ln_bias, w_out):
    layers, depth, chan = w_value.shape
    rows, dblk = inputs.shape
    width = w_out.shape[2]
    n_chunks = rows // CHUNK
    features = dblk * n_tp
    bf16, f32 = jnp.bfloat16, jnp.float32
    dma = pltpu.SemaphoreType.DMA
    vmem = pl.BlockSpec(memory_space=pltpu.VMEM)
    return pl.pallas_call(
        functools.partial(fused_kernel, n_sp, n_tp, 1e-06),
        out_shape=jax.ShapeDtypeStruct((rows, dblk), bf16),
        in_specs=[vmem] * 8,
        out_specs=vmem,
        scratch_shapes=[
            pltpu.VMEM((layers, n_sp * depth, chan), bf16),
            pltpu.VMEM((layers, n_sp * depth, chan), bf16),
            pltpu.VMEM((layers, PAIR, n_tp * chan, width), bf16),
            pltpu.VMEM((n_tp, rows, dblk), bf16),
            pltpu.VMEM((CHUNK, features), bf16),
            pltpu.VMEM((chan // LANES, HALO + rows, LANES), f32),
            pltpu.VMEM((rows, chan), f32),
            pltpu.VMEM((layers, HALO, chan), bf16),
            pltpu.VMEM((layers, HALO, chan), bf16),
            pltpu.VMEM((layers, n_chunks, n_tp, 8, CHUNK), f32),
            pltpu.VMEM((n_tp, rows, chan), bf16),
            dma((layers, PAIR, n_sp)),
            dma((layers, PAIR, n_sp // PAIR + 1)),
            dma((layers, PAIR, n_sp // PAIR)),
            dma((layers, n_tp, PAIR)),
            dma((layers, n_tp, 3)),
            dma((layers,)),
            dma((3, n_chunks)),
            dma((3, n_chunks)),
            dma((layers,)),
            dma((layers,)),
            dma((n_chunks, n_tp)),
            dma((n_chunks, n_tp)),
            dma((3, n_chunks)),
            dma((3, n_chunks)),
        ],
        compiler_params=pltpu.CompilerParams(collective_id=0, has_side_effects=True),
    )(
        inputs,
        norm_gain,
        w_value,
        w_gate,
        conv_taps,
        ln_gain,
        ln_bias,
        w_out,
    )


def fits_kernel(n_sp, n_tp, inputs, w_value, conv_taps, w_out):
    rows, dblk = inputs.shape
    width = w_out.shape[2]
    return (
        n_sp == 4 * PAIR
        and n_tp == PAIR * PAIR
        and rows % CHUNK == 0
        and rows // CHUNK >= 4
        and w_value.shape[0] >= 2
        and w_value.shape[1] % LANES == 0
        and w_value.shape[2] % LANES == 0
        and width % LANES == 0
        and dblk == PAIR * width
        and conv_taps.shape[1] - 1 <= HALO
    )


def shards(inputs, norm_gain, w_value, w_gate, conv_taps, ln_gain, ln_bias, w_out):
    n_sp, n_tp = lax.axis_size("sp"), lax.axis_size("tp")
    args = (inputs, norm_gain, w_value, w_gate, conv_taps, ln_gain, ln_bias, w_out)
    if fits_kernel(n_sp, n_tp, inputs, w_value, conv_taps, w_out):
        return fused_shards(n_sp, n_tp, *args)
    return plain_shards(*args)


def from_behind(block, axis, distance):
    devices = range(lax.axis_size(axis))
    route = [(i - distance, i) for i in devices if i - distance in devices]
    return lax.ppermute(block, axis, route)


def plain_shards(inputs, norm_gain, w_value, w_gate, conv_taps, ln_gain, ln_bias, w_out):
    rows = inputs.shape[0]
    reach = conv_taps.shape[1] - 1
    layers = conv_taps.shape[0]
    channels = conv_taps.shape[2] * lax.axis_size("tp")
    whole_value, whole_gate, whole_out = (
        lax.all_gather(w_value, "sp", axis=1, tiled=True),
        lax.all_gather(w_gate, "sp", axis=1, tiled=True),
        lax.all_gather(w_out, "sp", axis=2, tiled=True),
    )
    stream = inputs
    for layer in range(layers):
        full_rows = lax.all_gather(stream, "tp", axis=1, tiled=True)
        xf = full_rows.astype(jnp.float32)
        meansq = jnp.mean(xf * xf, axis=1, keepdims=True)
        hidden = (xf * lax.rsqrt(meansq + 1e-06) * norm_gain[layer][None, :]).astype(jnp.bfloat16)
        value = jnp.dot(hidden, whole_value[layer], preferred_element_type=jnp.float32)
        gate = jnp.dot(hidden, whole_gate[layer], preferred_element_type=jnp.float32)
        glu = (value * jax.nn.sigmoid(gate)).astype(jnp.bfloat16)
        rim = from_behind(glu[rows - reach :], "sp", 1)
        padded = jnp.concatenate([rim, glu], axis=0)
        count = padded.shape[0] - reach
        filtered = jnp.zeros((count, glu.shape[1]), jnp.float32)
        for tap in range(reach + 1):
            filtered = filtered + conv_taps[layer, tap][None, :] * padded[tap : tap + count].astype(
                jnp.float32
            )
        total_sum, total_sq = lax.psum(
            (jnp.sum(filtered, axis=1), jnp.sum(filtered * filtered, axis=1)), "tp"
        )
        mean_val = (total_sum / channels)[:, None]
        var_val = (total_sq / channels)[:, None] - mean_val * mean_val
        normed = jax.nn.silu(
            (filtered - mean_val) * lax.rsqrt(var_val + 1e-06) * ln_gain[layer][None, :]
            + ln_bias[layer][None, :]
        ).astype(jnp.bfloat16)
        partial_out = jnp.dot(normed, whole_out[layer], preferred_element_type=jnp.float32)
        summed = lax.psum_scatter(
            partial_out.astype(jnp.bfloat16), "tp", scatter_dimension=1, tiled=True
        ).astype(jnp.float32)
        kept = stream.astype(jnp.float32)
        stream = (kept + summed).astype(jnp.bfloat16)
    return stream


def solution(mesh):
    in_specs = (
        P("sp", "tp"),
        P(),
        P(None, "sp", "tp"),
        P(None, "sp", "tp"),
        P(None, None, "tp"),
        P(None, "tp"),
        P(None, "tp"),
        P(None, "tp", "sp"),
    )
    out_specs = P("sp", "tp")
    return jax.shard_map(shards, mesh=mesh, in_specs=in_specs, out_specs=out_specs, check_vma=False)
```

```python
import functools

import jax
import jax.numpy as jnp
from jax import lax
from jax.experimental import pallas as pl
from jax.experimental.pallas import tpu as pltpu
from jax.sharding import PartitionSpec as P

MESH = pl.DeviceIdType.MESH
PAIR = 2
CHUNK = 128
HALO = 32
LANES = 128
V, G, O, UP, OVER, ZOWN, XOWN, BEFORE, SIDE = 0, 1, 2, 3, 4, 5, 6, 7, 8
OWN_X = ((XOWN, V, 1), (XOWN, G, 1))
OWN_Z = ((ZOWN, V, 1), (ZOWN, G, 1))
RISEN, FIRST = -1, -2
LAST_X = ((XOWN, V, 2), (XOWN, G, 2))
LAST_Z = ((ZOWN, V, 2), (ZOWN, G, 2))


def every(kind, later):
    return tuple((kind, j, later) for j in range(4))


END_OPEN = (
    (V, 0, 0), *OWN_Z, (G, 0, 0), (V, 1, 0), (BEFORE, 0, 0), (G, 1, 0), (V, 2, 0), (G, 2, 0), (O, 0, 0),
    (XOWN, V, 1),
)
HEAD_OPEN = (
    (V, 0, 0), *every(UP, 0), *OWN_Z, (G, 0, 0), (V, 1, 0), (BEFORE, 0, 0), (G, 1, 0), (V, 2, 0), (G, 2, 0),
    *every(OVER, 0), *OWN_X,
)
MID_OPEN = (
    (V, 0, 0), (V, 1, 0), (G, 0, 0), (G, 1, 0), (V, 2, 0), (BEFORE, 0, 0), (G, 2, 0),
    (O, 0, 0), (O, 1, 0), (ZOWN, V, 1), (O, 2, 0),
)
NEAR_OPEN = (
    (V, 0, 0), (V, 1, 0), (G, 0, 0), (G, 1, 0), (V, 2, 0), (BEFORE, 0, 0), (G, 2, 0),
    *every(O, 0), *OWN_Z, *OWN_X,
)
END_PLAN = {
    1: ((O, 0, RISEN), (O, 1, 0)), 2: ((O, 2, 0), (XOWN, G, 1)), 3: ((O, 3, 0),), 5: ((V, 0, 1), *LAST_Z),
    6: ((V, 1, 1),), 7: ((V, 2, 1),), 8: ((G, 0, 1), (SIDE, 0, 1)), 9: ((G, 1, 1),), 10: ((G, 2, 1),),
    12: ((XOWN, V, 2),),
}
HEAD_PLAN = {
    3: every(UP, 1), 5: ((V, 0, 1), *LAST_Z), 6: ((V, 1, 1),), 7: ((V, 2, 1),),
    8: ((G, 0, 1), (SIDE, 0, 1)), 9: ((G, 1, 1),), 10: ((G, 2, 1), *every(OVER, 1), *LAST_X),
}
MID_PLAN = {
    1: ((O, 3, FIRST), (ZOWN, G, 1), *OWN_X), 3: ((V, 0, 1),), 4: ((V, 1, 1), (V, 2, 1)),
    5: ((G, 0, 1),), 6: ((G, 1, 1),), 7: ((G, 2, 1), (SIDE, 0, 1)),
    9: ((O, 0, 1),), 10: ((O, 1, 1),), 11: ((O, 2, 1),), 12: ((O, 3, 1), (ZOWN, V, 2)),
}
ROOT_PLAN = {
    1: ((V, 0, 1),), 2: ((V, 1, 1),), 3: ((V, 2, 1),), 4: ((G, 0, 1),), 5: ((G, 1, 1),),
    6: ((G, 2, 1),), 7: ((SIDE, 0, 1), (O, 0, 1), (O, 1, 1)), 8: ((O, 2, 1), (O, 3, 1), *LAST_Z, *LAST_X),
}
NEXT_PLAN = {
    1: ((V, 0, 1),), 2: ((V, 1, 1),), 3: ((V, 2, 1),), 4: ((G, 0, 1), (UP, 0, 1)), 5: ((G, 1, 1), (UP, 1, 1)),
    6: ((G, 2, 1), (UP, 2, 1)), 7: ((SIDE, 0, 1), (UP, 3, 1)),
    8: (*every(OVER, 1), *LAST_Z, *LAST_X),
}


def fused_kernel(
    n_sp, n_tp, eps,
    x_ref, gain_hbm, wv_ref, wg_ref, taps_hbm, lng_hbm, lnb_hbm, wo_ref,
    out_ref,
    gain_ref, taps_ref, lng_ref, lnb_ref, out_all, wv_all, wg_all, wo_all, xf, hid, glu, filt, stat, nrm,
    w_recv, w_zsend, w_xsend, o_recv, o_send, og_send,
    ag_recv, ag_send, before_s, before_r, st_recv, st_send, nr_recv, nr_send,
    in_sem, small_sem, out_sem,
):
    sp = lax.axis_index("sp")
    tp = lax.axis_index("tp")
    layers, depth = wv_ref.shape[0], wv_ref.shape[1]
    rows, dblk = x_ref.shape
    width = wo_ref.shape[2]
    chan = wv_ref.shape[2]
    taps = taps_ref.shape[1]
    features = dblk * n_tp
    channels = chan * n_tp
    n_chunks = rows // CHUNK
    n_out = n_sp // PAIR
    outer, inner = lax.div(sp, PAIR), lax.rem(sp, PAIR)
    x_peer = outer * PAIR + (PAIR - 1 - inner)
    far_half, core = lax.div(tp, PAIR), lax.rem(tp, PAIR)
    partner = far_half * PAIR + (PAIR - 1 - core)
    far = (n_tp // PAIR - 1 - far_half) * PAIR + core
    first_off = HALO - (taps - 1)
    ext = HALO * layers
    halves = chan // LANES

    last = n_out - 1
    upper = lax.div(outer, n_out // 2)
    near_end = outer + upper * (last - 2 * outer)

    def line(j):
        near = j + 1 - (near_end if j == 0 else 0)
        return near + upper * (last - 2 * near)

    slant = sp + 2 * inner - 1
    has_slant = (slant >= 0) & (slant < n_sp)
    barrier = pltpu.get_barrier_semaphore()

    def greet(sp_to, tp_to):
        pl.semaphore_signal(barrier, inc=1, device_id=(sp_to, tp_to), device_id_type=MESH)

    greet(line(0) * PAIR + inner, tp)
    greet(x_peer, tp)
    for step in range(1, n_tp):
        greet(sp, lax.rem(tp + step, n_tp))

    @pl.when(near_end == 1)
    def _():
        greet(line(1) * PAIR + inner, tp)

    @pl.when(has_slant)
    def _():
        greet(slant, tp)

    def own_rows(s):
        return pl.ds(pl.multiple_of(s * depth, depth), depth)

    def o_slot(l, x, b):
        return wo_all.at[l, x, pl.ds(pl.multiple_of(b * chan, chan), chan), :]

    def load_weight(m, l):
        src, dst = ((wv_ref, wv_all), (wg_ref, wg_all))[m]
        return pltpu.make_async_copy(src.at[l], dst.at[l, own_rows(sp), :], in_sem.at[m, l])

    def load_out(l):
        return pltpu.make_async_copy(wo_ref.at[l], o_slot(l, inner, tp), in_sem.at[2, l])

    def load_rows():
        return pltpu.make_async_copy(x_ref, xf.at[tp, pl.ds(ext, rows), :], small_sem.at[4])

    smalls = [
        pltpu.make_async_copy(src, dst, small_sem.at[i])
        for i, (src, dst) in enumerate(
            ((gain_hbm, gain_ref), (taps_hbm, taps_ref), (lng_hbm, lng_ref), (lnb_hbm, lnb_ref)))
    ]
    for m in range(PAIR):
        load_weight(m, 0).start()
    load_rows().start()

    @pl.when(outer == tp)
    def _():
        for l in range(layers):
            load_out(l).start()

    for l in range(1, layers):
        for m in range(PAIR):
            load_weight(m, l).start()
    for small in smalls:
        small.start()

    glu[:, 0:HALO, :] = jnp.zeros((halves, HALO, LANES), jnp.float32)

    @pl.when(sp == 0)
    def _():
        xf[tp, 0:ext, :] = jnp.zeros((ext, dblk), jnp.bfloat16)


    for m in range(PAIR):
        load_weight(m, 0).wait()
    pl.semaphore_wait(barrier, 2 + n_tp - 1 + near_end + has_slant.astype(jnp.int32))

    def parts(c):
        own = (ext + c * CHUNK, CHUNK)
        return ((0, ext), own) if c == 0 else (own,)

    def chunk_rows(c, skip):
        return pl.ds(ext + c * CHUNK, CHUNK) if c else pl.ds(skip * HALO, ext - skip * HALO + CHUNK)

    def by_layer(c, l, f):
        if c or isinstance(l, int):
            f(0 if c else l)
        else:
            for k in range(layers):
                pl.when(l == k)(functools.partial(f, k))

    def stat_rows(c):
        return pl.ds(0, 8 * len(parts(c)))

    def remote(src, dst, send, recv, sp_to, tp_to):
        return pltpu.make_async_remote_copy(
            src_ref=src, dst_ref=dst, send_sem=send, recv_sem=recv,
            device_id=(sp_to, tp_to), device_id_type=MESH,
        )

    def w_slot(m, l, s):
        return (wv_all, wg_all)[m].at[l, own_rows(s), :]

    def z_copy(m, l, j):
        to = line(j) * PAIR + inner
        return remote(w_slot(m, l, sp), w_slot(m, l, sp), w_zsend.at[l, m, j], w_recv.at[l, m, sp], to, tp)

    def z_arrival(m, l, j):
        s = line(j) * PAIR + inner
        return remote(w_slot(m, l, s), w_slot(m, l, s), w_zsend.at[l, m, j], w_recv.at[l, m, s], s, tp)

    def z_forward(m, l, j):
        s = line(j) * PAIR + inner
        to = line(1 if j == 0 else 0) * PAIR + inner
        slot = w_slot(m, l, s)
        return remote(slot, slot, w_zsend.at[l, m, PAIR + j], w_recv.at[l, m, s], to, tp)

    def x_own(m, l):
        return remote(w_slot(m, l, sp), w_slot(m, l, sp), w_xsend.at[l, m, last], w_recv.at[l, m, sp], x_peer, tp)

    def x_copy(m, l, j):
        s = line(j) * PAIR + inner
        slot = w_slot(m, l, s)
        return remote(slot, slot, w_xsend.at[l, m, j], w_recv.at[l, m, s], x_peer, tp)

    def x_arrival(m, l, z):
        s = z * PAIR + (PAIR - 1 - inner)
        slot = w_slot(m, l, s)
        return remote(slot, slot, w_xsend.at[l, m, last], w_recv.at[l, m, s], x_peer, tp)

    def side_copy(m, l):
        to = line(0) * PAIR + inner
        slot = w_slot(m, l, x_peer)
        return remote(slot, slot, w_xsend.at[l, m, 0], w_recv.at[l, m, x_peer], to, tp)

    def z_own(m, l):
        z_copy(m, l, 0).start()

        @pl.when(near_end == 1)
        def _():
            z_copy(m, l, 1).start()

    def relay_piece(m, l, j, side):
        z_arrival(m, l, j).wait_recv()

        @pl.when(near_end == 1)
        def _():
            z_forward(m, l, j).start()

        if j or not side:
            x_copy(m, l, j).start()

    def relay_side(m, l):
        x_arrival(m, l, outer).wait_recv()
        side_copy(m, l).start()

    def w_ready(m, l):
        if m == 1:
            @pl.when(l == 0)
            def _():
                x_arrival(m, l, outer).wait_recv()
        else:
            x_arrival(m, l, outer).wait_recv()
        for j in range(last):
            x_arrival(m, l, line(j)).wait_recv()

    def o_gather(l):
        return remote(wo_ref.at[l], o_slot(l, inner, tp), og_send.at[l], o_recv.at[l, tp, inner], sp, outer)

    def o_hop(l, j, way, to):
        b = lax.rem(tp + j, n_tp)
        slot = o_slot(l, inner, b)
        return remote(slot, slot, o_send.at[l, j, way], o_recv.at[l, b, inner], to, tp)

    def o_arrival(l, b, x):
        slot = o_slot(l, x, b)
        return remote(slot, slot, o_send.at[l, 0, 0], o_recv.at[l, b, x], x_peer, tp)

    goes_up = (outer >= tp) & (outer < last)
    goes_down = (outer <= tp) & (outer > 0)

    def send_o(l):
        @pl.when(outer != tp)
        def _():
            o_gather(l).start()

    def o_arrived(l, j):
        if j == 0:
            @pl.when(outer != tp)
            def _():
                o_arrival(l, tp, inner).wait_recv()
        else:
            o_arrival(l, lax.rem(tp + j, n_tp), inner).wait_recv()

    def o_along(l, j):
        @pl.when(goes_up)
        def _():
            o_hop(l, j, 0, sp + PAIR).start()

        @pl.when(goes_down)
        def _():
            o_hop(l, j, 1, sp - PAIR).start()

    def relay_o(l, j, kind):
        if kind != OVER:
            o_arrived(l, j)
            o_along(l, j)
        if kind != UP:
            o_hop(l, j, 2, x_peer).start()

    def o_ready(l):
        for j in range(n_tp):
            o_arrival(l, lax.rem(tp + j, n_tp), PAIR - 1 - inner).wait_recv()

    def ag_far(c, l):
        r = chunk_rows(c, l)
        return remote(xf.at[tp, r, :], xf.at[tp, r, :], ag_send.at[0, c], ag_recv.at[0, c], sp, far)

    def ag_partner(c, l):
        r = chunk_rows(c, l)
        return remote(xf.at[tp, r, :], xf.at[tp, r, :], ag_send.at[1, c], ag_recv.at[1, c], sp, partner)

    def ag_forward(c, l):
        r = chunk_rows(c, l)
        return remote(xf.at[far, r, :], xf.at[far, r, :], ag_send.at[2, c], ag_recv.at[2, c], sp, partner)

    def nr_far(c, l):
        r = chunk_rows(c, l + 1)
        return remote(nrm.at[tp, r, :], nrm.at[tp, r, :], nr_send.at[0, c], nr_recv.at[0, c], sp, far)

    def nr_partner(c, l):
        r = chunk_rows(c, l + 1)
        return remote(nrm.at[tp, r, :], nrm.at[tp, r, :], nr_send.at[1, c], nr_recv.at[1, c], sp, partner)

    def nr_forward(c, l):
        r = chunk_rows(c, l + 1)
        return remote(nrm.at[far, r, :], nrm.at[far, r, :], nr_send.at[2, c], nr_recv.at[2, c], sp, partner)

    def stat_copy(l, c, step):
        to = lax.rem(tp + step, n_tp)
        return remote(stat.at[l, c, tp, stat_rows(c), :], stat.at[l, c, tp, stat_rows(c), :], st_send.at[c, step], st_recv.at[c, tp], sp, to)

    def stat_arrival(l, c, step):
        src = lax.rem(tp + step, n_tp)
        return remote(stat.at[l, c, src, stat_rows(c), :], stat.at[l, c, src, stat_rows(c), :], st_send.at[c, step], st_recv.at[c, src], sp, src)

    def before_copy():
        to = lax.rem(sp + 1, n_sp)
        return remote(x_ref.at[pl.ds(rows - ext, ext), :], xf.at[tp, pl.ds(0, ext), :], before_s.at[0], before_r.at[0], to, tp)

    def do_pass(l, c):
        def go(k):
            ag_far(c, k).wait_recv()
            ag_forward(c, k).start()

        by_layer(c, l, go)

    def ag_start(l, c):
        def go(k):
            ag_far(c, k).start()
            ag_partner(c, k).start()

        by_layer(c, l, go)

    def ag_sent(l, c):
        def go(k):
            ag_far(c, k).wait_send()
            ag_partner(c, k).wait_send()
            ag_forward(c, k).wait_send()

        by_layer(c, l, go)

    def ag_wait(l, c):
        def go(k):
            ag_partner(c, k).wait_recv()
            ag_forward(c, k).wait_recv()

        by_layer(c, l, go)

    def nr_start(l, c):
        def go(k):
            nr_far(c, k).start()
            nr_partner(c, k).start()

        by_layer(c, l, go)

    def nr_sent(l, c):
        def go(k):
            nr_far(c, k).wait_send()
            nr_partner(c, k).wait_send()
            nr_forward(c, k).wait_send()

        by_layer(c, l, go)

    def nr_wait(l, c):
        def go(k):
            nr_partner(c, k).wait_recv()
            nr_forward(c, k).wait_recv()

        by_layer(c, l, go)

    def do_glu(l, c):
        ag_wait(l, c)
        for start, size in parts(c):
            r = slice(start, start + size)
            blocks = [xf[b, r, :].astype(jnp.float32) for b in range(n_tp)]
            total = sum(jnp.sum(b * b, axis=1, keepdims=True) for b in blocks)
            scale = lax.rsqrt(total / features + eps)
            for b in range(n_tp):
                cols = slice(b * dblk, (b + 1) * dblk)
                hid[0:size, cols] = (
                    xf[b, r, :].astype(jnp.float32) * scale * gain_ref[pl.ds(l, 1), cols]).astype(jnp.bfloat16)
            h = hid[0:size, :]
            value = jnp.dot(h, wv_all[l], preferred_element_type=jnp.float32)
            gate = jnp.dot(h, wg_all[l], preferred_element_type=jnp.float32)
            g = (value * jax.nn.sigmoid(gate)).astype(jnp.bfloat16).astype(jnp.float32)
            if start < ext:
                g = jnp.where(sp > 0, g, 0.0)
            for k in range(halves):
                glu[k, HALO + start:HALO + start + size, :] = g[:, k * LANES:(k + 1) * LANES]

    def do_conv(l, c):
        for i, (start, size) in enumerate(parts(c)):
            sums = jnp.zeros((size, 1), jnp.float32)
            squares = jnp.zeros((size, 1), jnp.float32)
            for k in range(halves):
                acc = jnp.zeros((size, LANES), jnp.float32)
                for tap in range(taps):
                    acc = acc + taps_ref[l, tap:tap + 1, k * LANES:(k + 1) * LANES] * glu[
                        k, start + first_off + tap:start + first_off + tap + size, :]
                filt[start:start + size, k * LANES:(k + 1) * LANES] = acc
                sums = sums + jnp.sum(acc, axis=1, keepdims=True)
                squares = squares + jnp.sum(acc * acc, axis=1, keepdims=True)
            lane = lax.broadcasted_iota(jnp.int32, (size, LANES), 1)
            both = jnp.where(lane == 0, sums, squares)
            if size < CHUNK:
                both = jnp.concatenate([both, jnp.zeros((CHUNK - size, LANES), jnp.float32)], axis=0)
            stat[l, c, tp, 8 * i:8 * i + 8, :] = jnp.transpose(both)[0:8, :]
        for step in range(1, n_tp):
            stat_copy(l, c, step).start()

    def do_norm(l, c):
        for step in range(1, n_tp):
            stat_arrival(l, c, step).wait_recv()
        def norm_part(i, start, size):
            r = slice(start, start + size)
            tot = stat[l, c, 0, 8 * i:8 * i + 8, :]
            for b in range(1, n_tp):
                tot = tot + stat[l, c, b, 8 * i:8 * i + 8, :]
            tot = jnp.transpose(jnp.concatenate([tot, jnp.zeros((LANES - 8, CHUNK), jnp.float32)], axis=0))
            mean = tot[0:size, 0:1] / channels
            var = tot[0:size, 1:2] / channels - mean * mean
            pre = (filt[r, :] - mean) * lax.rsqrt(var + eps) * lng_ref[pl.ds(l, 1), :] + lnb_ref[pl.ds(l, 1), :]
            nrm[tp, r, :] = jax.nn.silu(pre).astype(jnp.bfloat16)

        for i, (start, size) in enumerate(parts(c)):
            pl.when((start >= ext) | (l < layers - 1))(functools.partial(norm_part, i, start, size))
        ag_sent(l, c)
        for step in range(1, n_tp):
            stat_copy(l, c, step).wait_send()
        nr_start(l, c)

    def do_hand(l, c):
        def go(k):
            nr_far(c, k).wait_recv()
            nr_forward(c, k).start()

        by_layer(c, l, go)

    def store_rows(c):
        r = pl.ds(c * CHUNK, CHUNK)
        return pltpu.make_async_copy(out_all.at[r, :], out_ref.at[r, :], out_sem.at[c])

    def do_out(l, c):
        nr_wait(l, c)
        def out_part(start, size):
            r = slice(start, start + size)
            full = jnp.concatenate([nrm[b, r, :] for b in range(n_tp)], axis=1)
            for q in range(PAIR):
                cols = slice(q * width, (q + 1) * width)
                branch = jnp.dot(full, wo_all[l, q], preferred_element_type=jnp.float32)
                new = (xf[tp, r, cols].astype(jnp.float32) + branch).astype(jnp.bfloat16)
                xf[tp, r, cols] = new
                if start >= ext:
                    out_all[start - ext:start - ext + size, cols] = new

        for start, size in parts(c):
            pl.when((start >= ext) | (l < layers - 1))(functools.partial(out_part, start, size))

        @pl.when(l < layers - 1)
        def _():
            ag_start(l + 1, c)

        @pl.when(l == layers - 1)
        def _():
            store_rows(c).start()

        nr_sent(l, c)

    by_head = near_end * (outer - tp) * (outer - tp) * (1 - (far_half - core) * (far_half - core)) == 1
    is_root = (near_end == 1) & (outer == tp)
    is_mid = (near_end == 1) & (outer != tp) & jnp.logical_not(by_head)
    is_head = (near_end == 0) & (outer == tp)
    is_end = (near_end == 0) & (outer != tp)

    roles = (
        (is_end, END_OPEN, END_PLAN), (is_head, HEAD_OPEN, HEAD_PLAN),
        (is_mid, MID_OPEN, MID_PLAN), (is_root, NEAR_OPEN, ROOT_PLAN), (by_head, NEAR_OPEN, NEXT_PLAN),
    )

    def act(kind, j, l, side):
        if kind == BEFORE:
            @pl.when(sp > 0)
            def _():
                before_copy().wait_recv()

            ag_start(0, 0)
        elif kind == SIDE:
            relay_side(G, l)
        elif kind == ZOWN:
            z_own(j, l)
        elif kind == XOWN:
            x_own(j, l).start()
        elif kind >= O:
            relay_o(l, j, kind)
        else:
            relay_piece(kind, l, j, side and kind == G)

    for m in (V, G):
        z_own(m, 0)
        x_own(m, 0).start()
    @pl.when(sp < n_sp - 1)
    def _():
        before_copy().start()

    send_o(0)
    load_rows().wait()
    for c in range(1, n_chunks):
        ag_start(0, c)
    for l in range(1, layers):
        for m in range(PAIR):
            load_weight(m, l).wait()

    @pl.when(outer == tp)
    def _():
        for l in range(layers):
            load_out(l).wait()

    for small in smalls:
        small.wait()
    for role, order, _ in roles:
        @pl.when(role)
        def _():
            for kind, j, later in order:
                act(kind, j, later, False)

    for c in range(n_chunks):
        do_pass(0, c)
    w_ready(V, 0)
    w_ready(G, 0)

    def layer_body(l, carry):
        more = l < layers - 1

        def ahead(f):
            pl.when(more)(f)

        def slot(n):
            for role, _, plan in roles:
                for kind, j, later in plan.get(n, ()):
                    if later == RISEN:
                        when = role & (l > 0)
                    elif later == FIRST:
                        when = role & (l == 0)
                    else:
                        when = (role & (l + later < layers)) if later else role

                    @pl.when(when)
                    def _():
                        act(kind, j, l + max(later, 0), True)

        def pass_next(c):
            ahead(lambda: do_pass(l + 1, c))

        do_glu(l, 0)
        do_conv(l, 0)
        ahead(lambda: send_o(l + 1))
        slot(1)
        do_glu(l, 1)
        do_conv(l, 1)
        do_glu(l, 2)
        do_conv(l, 2)
        slot(2)
        do_norm(l, 0)
        do_glu(l, 3)
        do_conv(l, 3)
        do_norm(l, 1)
        slot(3)
        do_norm(l, 2)
        do_norm(l, 3)
        slot(4)
        do_hand(l, 0)
        slot(5)
        do_hand(l, 1)
        o_ready(l)
        do_out(l, 0)
        do_hand(l, 2)
        do_out(l, 1)
        slot(6)
        do_hand(l, 3)
        do_out(l, 2)
        slot(7)
        do_out(l, 3)
        slot(8)
        pass_next(0)
        slot(9)
        pass_next(1)
        slot(10)
        pass_next(2)
        slot(11)
        pass_next(3)
        slot(12)

        @pl.when(more)
        def _():
            w_ready(V, l + 1)
            w_ready(G, l + 1)

        return carry

    lax.fori_loop(0, layers, layer_body, 0)

    def drain(l, carry):
        for m in range(PAIR):
            z_copy(m, l, 0).wait_send()

            @pl.when(near_end == 1)
            def _():
                z_copy(m, l, 1).wait_send()
                for j in range(last):
                    z_forward(m, l, j).wait_send()

            for j in range(last):
                x_copy(m, l, j).wait_send()
            x_own(m, l).wait_send()

        @pl.when(outer != tp)
        def _():
            o_gather(l).wait_send()

        for j in range(n_tp):
            @pl.when(goes_up)
            def _():
                o_hop(l, j, 0, sp + PAIR).wait_send()

            @pl.when(goes_down)
            def _():
                o_hop(l, j, 1, sp - PAIR).wait_send()

            o_hop(l, j, 2, x_peer).wait_send()

        return carry

    lax.fori_loop(0, layers, drain, 0)

    @pl.when(sp < n_sp - 1)
    def _():
        before_copy().wait_send()

    for c in range(n_chunks):
        store_rows(c).wait()


def fused_shards(n_sp, n_tp, inputs, norm_gain, w_value, w_gate, conv_taps, ln_gain, ln_bias, w_out):
    layers, depth, chan = w_value.shape
    rows, dblk = inputs.shape
    width = w_out.shape[2]
    n_chunks = rows // CHUNK
    features = dblk * n_tp
    ext = HALO * layers
    bf16, f32 = jnp.bfloat16, jnp.float32
    dma = pltpu.SemaphoreType.DMA
    place = pl.BlockSpec(memory_space=pl.ANY)
    return pl.pallas_call(
        functools.partial(fused_kernel, n_sp, n_tp, 1e-06),
        out_shape=jax.ShapeDtypeStruct((rows, dblk), bf16),
        in_specs=[place] * 8,
        out_specs=place,
        scratch_shapes=[
            pltpu.VMEM(norm_gain.shape, f32),
            pltpu.VMEM(conv_taps.shape, f32),
            pltpu.VMEM(ln_gain.shape, f32),
            pltpu.VMEM(ln_bias.shape, f32),
            pltpu.VMEM((rows, dblk), bf16),
            pltpu.VMEM((layers, n_sp * depth, chan), bf16),
            pltpu.VMEM((layers, n_sp * depth, chan), bf16),
            pltpu.VMEM((layers, PAIR, n_tp * chan, width), bf16),
            pltpu.VMEM((n_tp, ext + rows, dblk), bf16),
            pltpu.VMEM((CHUNK, features), bf16),
            pltpu.VMEM((chan // LANES, HALO + ext + rows, LANES), f32),
            pltpu.VMEM((ext + rows, chan), f32),
            pltpu.VMEM((layers, n_chunks, n_tp, 16, CHUNK), f32),
            pltpu.VMEM((n_tp, ext + rows, chan), bf16),
            dma((layers, PAIR, n_sp)),
            dma((layers, PAIR, n_sp // PAIR + 1)),
            dma((layers, PAIR, n_sp // PAIR)),
            dma((layers, n_tp, PAIR)),
            dma((layers, n_tp, 3)),
            dma((layers,)),
            dma((3, n_chunks)),
            dma((3, n_chunks)),
            dma((1,)),
            dma((1,)),
            dma((n_chunks, n_tp)),
            dma((n_chunks, n_tp)),
            dma((3, n_chunks)),
            dma((3, n_chunks)),
            dma((3, layers)),
            dma((5,)),
            dma((n_chunks,)),
        ],
        compiler_params=pltpu.CompilerParams(collective_id=0, has_side_effects=True),
    )(
        inputs,
        norm_gain,
        w_value,
        w_gate,
        conv_taps,
        ln_gain,
        ln_bias,
        w_out,
    )


def fits_kernel(n_sp, n_tp, inputs, w_value, conv_taps, w_out):
    rows, dblk = inputs.shape
    width = w_out.shape[2]
    return (
        n_sp == 4 * PAIR
        and n_tp == PAIR * PAIR
        and rows % CHUNK == 0
        and rows // CHUNK >= 4
        and w_value.shape[0] >= 2
        and w_value.shape[1] % LANES == 0
        and w_value.shape[2] % LANES == 0
        and width % LANES == 0
        and dblk == PAIR * width
        and conv_taps.shape[1] - 1 <= HALO
        and HALO * w_value.shape[0] <= CHUNK
        and rows // CHUNK == 4
    )


def shards(inputs, norm_gain, w_value, w_gate, conv_taps, ln_gain, ln_bias, w_out):
    n_sp, n_tp = lax.axis_size("sp"), lax.axis_size("tp")
    args = (inputs, norm_gain, w_value, w_gate, conv_taps, ln_gain, ln_bias, w_out)
    if fits_kernel(n_sp, n_tp, inputs, w_value, conv_taps, w_out):
        return fused_shards(n_sp, n_tp, *args)
    return plain_shards(*args)


def from_behind(block, axis, distance):
    devices = range(lax.axis_size(axis))
    route = [(i - distance, i) for i in devices if i - distance in devices]
    return lax.ppermute(block, axis, route)


def plain_shards(inputs, norm_gain, w_value, w_gate, conv_taps, ln_gain, ln_bias, w_out):
    rows = inputs.shape[0]
    reach = conv_taps.shape[1] - 1
    layers = conv_taps.shape[0]
    channels = conv_taps.shape[2] * lax.axis_size("tp")
    whole_value, whole_gate, whole_out = (
        lax.all_gather(w_value, "sp", axis=1, tiled=True),
        lax.all_gather(w_gate, "sp", axis=1, tiled=True),
        lax.all_gather(w_out, "sp", axis=2, tiled=True),
    )
    stream = inputs
    for layer in range(layers):
        full_rows = lax.all_gather(stream, "tp", axis=1, tiled=True)
        xf = full_rows.astype(jnp.float32)
        meansq = jnp.mean(xf * xf, axis=1, keepdims=True)
        hidden = (xf * lax.rsqrt(meansq + 1e-06) * norm_gain[layer][None, :]).astype(jnp.bfloat16)
        value = jnp.dot(hidden, whole_value[layer], preferred_element_type=jnp.float32)
        gate = jnp.dot(hidden, whole_gate[layer], preferred_element_type=jnp.float32)
        glu = (value * jax.nn.sigmoid(gate)).astype(jnp.bfloat16)
        rim = from_behind(glu[rows - reach :], "sp", 1)
        padded = jnp.concatenate([rim, glu], axis=0)
        count = padded.shape[0] - reach
        filtered = jnp.zeros((count, glu.shape[1]), jnp.float32)
        for tap in range(reach + 1):
            filtered = filtered + conv_taps[layer, tap][None, :] * padded[tap : tap + count].astype(
                jnp.float32
            )
        total_sum, total_sq = lax.psum(
            (jnp.sum(filtered, axis=1), jnp.sum(filtered * filtered, axis=1)), "tp"
        )
        mean_val = (total_sum / channels)[:, None]
        var_val = (total_sq / channels)[:, None] - mean_val * mean_val
        normed = jax.nn.silu(
            (filtered - mean_val) * lax.rsqrt(var_val + 1e-06) * ln_gain[layer][None, :]
            + ln_bias[layer][None, :]
        ).astype(jnp.bfloat16)
        partial_out = jnp.dot(normed, whole_out[layer], preferred_element_type=jnp.float32)
        summed = lax.psum_scatter(
            partial_out.astype(jnp.bfloat16), "tp", scatter_dimension=1, tiled=True
        ).astype(jnp.float32)
        kept = stream.astype(jnp.float32)
        stream = (kept + summed).astype(jnp.bfloat16)
    return stream


def solution(mesh):
    in_specs = (
        P("sp", "tp"),
        P(),
        P(None, "sp", "tp"),
        P(None, "sp", "tp"),
        P(None, None, "tp"),
        P(None, "tp"),
        P(None, "tp"),
        P(None, "tp", "sp"),
    )
    out_specs = P("sp", "tp")
    return jax.shard_map(shards, mesh=mesh, in_specs=in_specs, out_specs=out_specs, check_vma=False)
```

```python
import functools

import jax
import jax.numpy as jnp
from jax import lax
from jax.experimental import pallas as pl
from jax.experimental.pallas import tpu as pltpu
from jax.sharding import PartitionSpec as P

MESH = pl.DeviceIdType.MESH
PAIR = 2
CHUNK = 128
HALO = 32
LANES = 128
V, G, O, UP, OVER, ZOWN, XOWN, BEFORE, SIDE = 0, 1, 2, 3, 4, 5, 6, 7, 8
OWN_X = ((XOWN, V, 1), (XOWN, G, 1))
OWN_Z = ((ZOWN, V, 1), (ZOWN, G, 1))
FIRST, MIDDLE, RISEN, CLOSING = 0, 1, 2, 3
LAST_X = ((XOWN, V, 2), (XOWN, G, 2))
LAST_Z = ((ZOWN, V, 2), (ZOWN, G, 2))


def every(kind, later):
    return tuple((kind, j, later) for j in range(4))


END_OPEN = (
    (V, 0, 0), *OWN_Z, (G, 0, 0), (V, 1, 0), (BEFORE, 0, 0), (G, 1, 0), (V, 2, 0), (G, 2, 0), (O, 0, 0),
    (XOWN, V, 1),
)
HEAD_OPEN = (
    (V, 0, 0), *every(UP, 0), *OWN_Z, (G, 0, 0), (V, 1, 0), (BEFORE, 0, 0), (G, 1, 0), (V, 2, 0), (G, 2, 0),
    *every(OVER, 0), *OWN_X,
)
MID_OPEN = (
    (V, 0, 0), (V, 1, 0), (G, 0, 0), (G, 1, 0), (V, 2, 0), (BEFORE, 0, 0), (G, 2, 0),
    (O, 0, 0), (O, 1, 0), (ZOWN, V, 1), (O, 2, 0),
)
NEAR_OPEN = (
    (V, 0, 0), (V, 1, 0), (G, 0, 0), (G, 1, 0), (V, 2, 0), (BEFORE, 0, 0), (G, 2, 0),
    *every(O, 0), *OWN_Z, *OWN_X,
)
END_PLAN = {
    1: ((O, 0, 0, RISEN), (O, 1, 0)), 2: ((O, 2, 0),), 3: ((O, 3, 0), (XOWN, G, 1)), 4: ((V, 0, 1), *LAST_Z),
    13: ((G, 0, 1, FIRST), (V, 1, 1, FIRST), (V, 2, 1, FIRST)),
    6: ((V, 1, 1, RISEN),), 7: ((V, 2, 1, RISEN), (SIDE, V, 1)), 8: ((G, 0, 1, RISEN), (SIDE, G, 1)),
    9: ((G, 1, 1),), 10: ((G, 2, 1),), 12: ((XOWN, V, 2),),
}
HEAD_PLAN = {
    3: every(UP, 1), 5: ((V, 0, 1), *LAST_Z), 6: ((V, 1, 1),), 7: ((V, 2, 1), (SIDE, V, 1)),
    8: ((G, 0, 1), (SIDE, G, 1)), 9: ((G, 1, 1),), 10: ((G, 2, 1), *every(OVER, 1), *LAST_X),
}
MID_PLAN = {
    1: ((O, 3, 0, FIRST), (ZOWN, G, 1), *OWN_X), 2: ((V, 0, 1), (V, 1, 1)), 3: ((V, 2, 1),), 4: ((G, 0, 1), (SIDE, V, 1)),
    5: ((G, 1, 1),), 6: ((G, 2, 1),), 7: ((SIDE, G, 1),),
    9: ((O, 0, 1),), 10: ((O, 1, 1),), 11: ((O, 2, 1),), 12: ((O, 3, 1), (ZOWN, V, 2)),
}
ROOT_PLAN = {
    1: ((V, 0, 1),), 2: ((V, 1, 1),), 3: ((V, 2, 1),), 4: ((G, 0, 1),), 5: ((G, 1, 1), (SIDE, V, 1)),
    6: ((G, 2, 1),), 7: ((SIDE, G, 1), (O, 0, 1), (O, 1, 1)), 8: ((O, 2, 1), (O, 3, 1), *LAST_Z, *LAST_X),
}
NEXT_PLAN = {
    1: ((V, 0, 1),), 2: ((V, 1, 1),), 3: ((V, 2, 1),), 4: ((G, 0, 1), (UP, 0, 1)), 5: ((G, 1, 1), (UP, 1, 1), (SIDE, V, 1)),
    6: ((G, 2, 1), (UP, 2, 1)), 7: ((SIDE, G, 1), (UP, 3, 1)),
    8: (*every(OVER, 1), *LAST_Z, *LAST_X),
}


def fused_kernel(
    n_sp, n_tp, eps,
    x_ref, gain_hbm, wv_ref, wg_ref, taps_hbm, lng_hbm, lnb_hbm, wo_ref,
    out_ref,
    gain_ref, taps_ref, lng_ref, lnb_ref, out_all, wv_all, wg_all, wo_all, xf, hid, glu, filt, stat, nrm,
    w_recv, w_xrecv, w_zsend, w_xsend, o_recv, o_xrecv, o_send, og_send,
    ag_recv, ag_send, before_s, before_r, st_recv, st_send, nr_recv, nr_send,
    in_sem, small_sem, out_sem,
):
    sp = lax.axis_index("sp")
    tp = lax.axis_index("tp")
    layers, depth = wv_ref.shape[0], wv_ref.shape[1]
    rows, dblk = x_ref.shape
    width = wo_ref.shape[2]
    chan = wv_ref.shape[2]
    taps = taps_ref.shape[1]
    features = dblk * n_tp
    channels = chan * n_tp
    n_chunks = rows // CHUNK
    n_out = n_sp // PAIR
    outer, inner = lax.div(sp, PAIR), lax.rem(sp, PAIR)
    x_peer = outer * PAIR + (PAIR - 1 - inner)
    far_half, core = lax.div(tp, PAIR), lax.rem(tp, PAIR)
    partner = far_half * PAIR + (PAIR - 1 - core)
    far = (n_tp // PAIR - 1 - far_half) * PAIR + core
    first_off = HALO - (taps - 1)
    ext = HALO * layers
    halves = chan // LANES

    last = n_out - 1
    upper = lax.div(outer, n_out // 2)
    near_end = outer + upper * (last - 2 * outer)

    def line(j):
        near = j + 1 - (near_end if j == 0 else 0)
        return near + upper * (last - 2 * near)

    slant = sp + 2 * inner - 1
    has_slant = (slant >= 0) & (slant < n_sp)
    barrier = pltpu.get_barrier_semaphore()

    def greet(sp_to, tp_to):
        pl.semaphore_signal(barrier, inc=1, device_id=(sp_to, tp_to), device_id_type=MESH)

    greet(line(0) * PAIR + inner, tp)
    greet(x_peer, tp)
    for step in range(1, n_tp):
        greet(sp, lax.rem(tp + step, n_tp))

    @pl.when(near_end == 1)
    def _():
        greet(line(1) * PAIR + inner, tp)

    @pl.when(has_slant)
    def _():
        greet(slant, tp)

    def own_rows(s):
        return pl.ds(pl.multiple_of(s * depth, depth), depth)

    def o_slot(l, x, b):
        return wo_all.at[l, x, pl.ds(pl.multiple_of(b * chan, chan), chan), :]

    def load_weight(m, l):
        src, dst = ((wv_ref, wv_all), (wg_ref, wg_all))[m]
        return pltpu.make_async_copy(src.at[l], dst.at[l, own_rows(sp), :], in_sem.at[m, l])

    def load_out(l):
        return pltpu.make_async_copy(wo_ref.at[l], o_slot(l, inner, tp), in_sem.at[2, l])

    def load_rows():
        return pltpu.make_async_copy(x_ref, xf.at[tp, pl.ds(ext, rows), :], small_sem.at[4])

    smalls = [
        pltpu.make_async_copy(src, dst, small_sem.at[i])
        for i, (src, dst) in enumerate(
            ((gain_hbm, gain_ref), (taps_hbm, taps_ref), (lng_hbm, lng_ref), (lnb_hbm, lnb_ref)))
    ]
    for m in range(PAIR):
        load_weight(m, 0).start()
    load_rows().start()

    @pl.when(outer == tp)
    def _():
        for l in range(layers):
            load_out(l).start()

    for l in range(1, layers):
        for m in range(PAIR):
            load_weight(m, l).start()
    for small in smalls:
        small.start()

    glu[:, 0:HALO, :] = jnp.zeros((halves, HALO, LANES), jnp.float32)

    @pl.when(sp == 0)
    def _():
        xf[tp, 0:ext, :] = jnp.zeros((ext, dblk), jnp.bfloat16)


    for m in range(PAIR):
        load_weight(m, 0).wait()
    pl.semaphore_wait(barrier, 2 + n_tp - 1 + near_end + has_slant.astype(jnp.int32))

    def parts(c):
        own = (ext + c * CHUNK, CHUNK)
        return ((0, ext), own) if c == 0 else (own,)

    def chunk_rows(c, skip):
        return pl.ds(ext + c * CHUNK, CHUNK) if c else pl.ds(skip * HALO, ext - skip * HALO + CHUNK)

    def by_layer(c, l, f):
        if c or isinstance(l, int):
            f(0 if c else l)
        else:
            for k in range(layers):
                pl.when(l == k)(functools.partial(f, k))

    def stat_rows(c):
        return pl.ds(0, 8 * len(parts(c)))

    def remote(src, dst, send, recv, sp_to, tp_to):
        return pltpu.make_async_remote_copy(
            src_ref=src, dst_ref=dst, send_sem=send, recv_sem=recv,
            device_id=(sp_to, tp_to), device_id_type=MESH,
        )

    def w_slot(m, l, s):
        return (wv_all, wg_all)[m].at[l, own_rows(s), :]

    def z_copy(m, l, j):
        to = line(j) * PAIR + inner
        return remote(w_slot(m, l, sp), w_slot(m, l, sp), w_zsend.at[m], w_recv.at[l, m, outer], to, tp)

    def z_arrival(m, l, j):
        s = line(j) * PAIR + inner
        return remote(w_slot(m, l, s), w_slot(m, l, s), w_zsend.at[m], w_recv.at[l, m, line(j)], s, tp)

    def z_forward(m, l, j):
        s = line(j) * PAIR + inner
        to = line(1 if j == 0 else 0) * PAIR + inner
        slot = w_slot(m, l, s)
        return remote(slot, slot, w_zsend.at[m], w_recv.at[l, m, line(j)], to, tp)

    def x_own(m, l):
        return remote(w_slot(m, l, sp), w_slot(m, l, sp), w_xsend.at[m], w_xrecv.at[l, m, 0], x_peer, tp)

    def x_copy(m, l, j):
        s = line(j) * PAIR + inner
        slot = w_slot(m, l, s)
        return remote(slot, slot, w_xsend.at[m], w_xrecv.at[l, m, 1], x_peer, tp)

    def x_arrival(m, l):
        slot = w_slot(m, l, x_peer)
        return remote(slot, slot, w_xsend.at[m], w_xrecv.at[l, m, 0], x_peer, tp)

    def x_arrivals(m, l):
        block = (wv_all, wg_all)[m].at[l, pl.ds(0, last * depth), :]
        return remote(block, block, w_xsend.at[m], w_xrecv.at[l, m, 1], x_peer, tp)

    def side_copy(m, l):
        to = line(0) * PAIR + inner
        slot = w_slot(m, l, x_peer)
        return remote(slot, slot, w_xsend.at[m], w_xrecv.at[l, m, 1], to, tp)

    def z_own(m, l):
        z_copy(m, l, 0).start()

        @pl.when(near_end == 1)
        def _():
            z_copy(m, l, 1).start()

    def relay_piece(m, l, j, side):
        z_arrival(m, l, j).wait_recv()

        @pl.when(near_end == 1)
        def _():
            z_forward(m, l, j).start()

        if j or not side:
            x_copy(m, l, j).start()
        elif m == V:
            @pl.when(jnp.logical_not(by_side(m, l)))
            def _():
                x_copy(m, l, j).start()

    def by_side(m, l):
        return l > 0 if m == G else (l > 0) & ((l < layers - 1) | (upper == far_half))

    def relay_side(m, l):
        @pl.when(by_side(m, l))
        def _():
            x_arrival(m, l).wait_recv()
            side_copy(m, l).start()

    def w_ready(m, l):
        @pl.when(jnp.logical_not(by_side(m, l)))
        def _():
            x_arrival(m, l).wait_recv()

        x_arrivals(m, l).wait_recv()

    def o_gather(l):
        return remote(wo_ref.at[l], o_slot(l, inner, tp), og_send.at[0], o_recv.at[l, tp], sp, outer)

    def o_hop(l, j, way, to):
        b = lax.rem(tp + j, n_tp)
        slot = o_slot(l, inner, b)
        return remote(slot, slot, o_send.at[way], o_xrecv.at[l] if way == 2 else o_recv.at[l, b], to, tp)

    def o_arrival(l, b):
        slot = o_slot(l, inner, b)
        return remote(slot, slot, o_send.at[0], o_recv.at[l, b], x_peer, tp)

    goes_up = (outer >= tp) & (outer < last)
    goes_down = (outer <= tp) & (outer > 0)

    def send_o(l):
        @pl.when(outer != tp)
        def _():
            o_gather(l).start()

    def o_arrived(l, j):
        if j == 0:
            @pl.when(outer != tp)
            def _():
                o_arrival(l, tp).wait_recv()
        else:
            o_arrival(l, lax.rem(tp + j, n_tp)).wait_recv()

    def o_along(l, j):
        @pl.when(goes_up)
        def _():
            o_hop(l, j, 0, sp + PAIR).start()

        @pl.when(goes_down)
        def _():
            o_hop(l, j, 1, sp - PAIR).start()

    def relay_o(l, j, kind):
        if kind != OVER:
            o_arrived(l, j)
            o_along(l, j)
        if kind != UP:
            o_hop(l, j, 2, x_peer).start()

    def o_ready(l):
        block = wo_all.at[l, 0]
        remote(block, block, o_send.at[2], o_xrecv.at[l], x_peer, tp).wait_recv()

    def ag_far(c, l):
        r = chunk_rows(c, l)
        return remote(xf.at[tp, r, :], xf.at[tp, r, :], ag_send.at[c], ag_recv.at[0, c], sp, far)

    def ag_partner(c, l):
        r = chunk_rows(c, l)
        return remote(xf.at[tp, r, :], xf.at[tp, r, :], ag_send.at[c], ag_recv.at[1, c], sp, partner)

    def ag_forward(c, l):
        r = chunk_rows(c, l)
        return remote(xf.at[far, r, :], xf.at[far, r, :], ag_send.at[c], ag_recv.at[1, c], sp, partner)

    def nr_far(c, l):
        r = chunk_rows(c, l + 1)
        return remote(nrm.at[tp, r, :], nrm.at[tp, r, :], nr_send.at[c], nr_recv.at[0, c], sp, far)

    def nr_partner(c, l):
        r = chunk_rows(c, l + 1)
        return remote(nrm.at[tp, r, :], nrm.at[tp, r, :], nr_send.at[c], nr_recv.at[1, c], sp, partner)

    def nr_forward(c, l):
        r = chunk_rows(c, l + 1)
        return remote(nrm.at[far, r, :], nrm.at[far, r, :], nr_send.at[c], nr_recv.at[1, c], sp, partner)

    def stat_copy(l, c, step):
        to = lax.rem(tp + step, n_tp)
        return remote(stat.at[l, c, tp, stat_rows(c), :], stat.at[l, c, tp, stat_rows(c), :], st_send.at[c], st_recv.at[c], sp, to)

    def stats(l, c):
        block = stat.at[l, c, pl.ds(0, n_tp - 1), stat_rows(c), :]
        return remote(block, block, st_send.at[c], st_recv.at[c], sp, far)

    def before_copy():
        to = lax.rem(sp + 1, n_sp)
        return remote(x_ref.at[pl.ds(rows - ext, ext), :], xf.at[tp, pl.ds(0, ext), :], before_s.at[0], before_r.at[0], to, tp)

    def do_pass(l, c):
        def go(k):
            ag_far(c, k).wait_recv()
            ag_forward(c, k).start()

        by_layer(c, l, go)

    def ag_start(l, c):
        def go(k):
            ag_far(c, k).start()
            ag_partner(c, k).start()

        by_layer(c, l, go)

    def ag_sent(l, c):
        def go(k):
            block = xf.at[pl.ds(0, 3), chunk_rows(c, k), :]
            remote(block, block, ag_send.at[c], ag_recv.at[1, c], sp, far).wait_send()

        by_layer(c, l, go)

    def ag_wait(l, c):
        def go(k):
            block = xf.at[pl.ds(0, PAIR), chunk_rows(c, k), :]
            remote(block, block, ag_send.at[c], ag_recv.at[1, c], sp, partner).wait_recv()

        by_layer(c, l, go)

    def nr_start(l, c):
        def go(k):
            nr_far(c, k).start()
            nr_partner(c, k).start()

        by_layer(c, l, go)

    def nr_sent(l, c):
        def go(k):
            block = nrm.at[pl.ds(0, 3), chunk_rows(c, k + 1), :]
            remote(block, block, nr_send.at[c], nr_recv.at[1, c], sp, far).wait_send()

        by_layer(c, l, go)

    def nr_wait(l, c):
        def go(k):
            block = nrm.at[pl.ds(0, PAIR), chunk_rows(c, k + 1), :]
            remote(block, block, nr_send.at[c], nr_recv.at[1, c], sp, partner).wait_recv()

        by_layer(c, l, go)

    def do_glu(l, cs):
        for c in cs:
            ag_wait(l, c)

        def glu_part(start, size):
            r = slice(start, start + size)
            blocks = [xf[b, r, :].astype(jnp.float32) for b in range(n_tp)]
            total = sum(jnp.sum(b * b, axis=1, keepdims=True) for b in blocks)
            scale = lax.rsqrt(total / features + eps)
            for b in range(n_tp):
                cols = slice(b * dblk, (b + 1) * dblk)
                hid[0:size, cols] = (
                    xf[b, r, :].astype(jnp.float32) * scale * gain_ref[pl.ds(l, 1), cols]).astype(jnp.bfloat16)
            h = hid[0:size, :]
            value = jnp.dot(h, wv_all[l], preferred_element_type=jnp.float32)
            gate = jnp.dot(h, wg_all[l], preferred_element_type=jnp.float32)
            g = (value * jax.nn.sigmoid(gate)).astype(jnp.bfloat16).astype(jnp.float32)
            if start < ext:
                row = lax.broadcasted_iota(jnp.int32, g.shape, 0)
                g = jnp.where((row >= ext - start) | (sp > 0), g, 0.0)
            for k in range(halves):
                glu[k, HALO + start:HALO + start + size, :] = g[:, k * LANES:(k + 1) * LANES]

        start, size = ext + cs[0] * CHUNK, len(cs) * CHUNK
        if cs[0]:
            glu_part(start, size)
        else:
            pl.when(l < layers - 1)(functools.partial(glu_part, 0, start + size))
            pl.when(l == layers - 1)(functools.partial(glu_part, ext - HALO, HALO + size))

    def do_conv(l, c):
        def conv_part(i, start, size):
            sums = jnp.zeros((size, 1), jnp.float32)
            squares = jnp.zeros((size, 1), jnp.float32)
            for k in range(halves):
                acc = jnp.zeros((size, LANES), jnp.float32)
                for tap in range(taps):
                    acc = acc + taps_ref[l, tap:tap + 1, k * LANES:(k + 1) * LANES] * glu[
                        k, start + first_off + tap:start + first_off + tap + size, :]
                filt[start:start + size, k * LANES:(k + 1) * LANES] = acc
                sums = sums + jnp.sum(acc, axis=1, keepdims=True)
                squares = squares + jnp.sum(acc * acc, axis=1, keepdims=True)
            lane = lax.broadcasted_iota(jnp.int32, (size, LANES), 1)
            both = jnp.where(lane == 0, sums, squares)
            if size < CHUNK:
                both = jnp.concatenate([both, jnp.zeros((CHUNK - size, LANES), jnp.float32)], axis=0)
            stat[l, c, tp, 8 * i:8 * i + 8, :] = jnp.transpose(both)[0:8, :]

        for i, (start, size) in enumerate(parts(c)):
            if start < ext:
                pl.when(l < layers - 1)(functools.partial(conv_part, i, start, size))
            else:
                conv_part(i, start, size)
        for step in range(1, n_tp):
            stat_copy(l, c, step).start()

    def do_norm(l, c):
        stats(l, c).wait_recv()

        def norm_part(i, start, size):
            r = slice(start, start + size)
            tot = stat[l, c, 0, 8 * i:8 * i + 8, :]
            for b in range(1, n_tp):
                tot = tot + stat[l, c, b, 8 * i:8 * i + 8, :]
            tot = jnp.transpose(jnp.concatenate([tot, jnp.zeros((LANES - 8, CHUNK), jnp.float32)], axis=0))
            mean = tot[0:size, 0:1] / channels
            var = tot[0:size, 1:2] / channels - mean * mean
            pre = (filt[r, :] - mean) * lax.rsqrt(var + eps) * lng_ref[pl.ds(l, 1), :] + lnb_ref[pl.ds(l, 1), :]
            nrm[tp, r, :] = jax.nn.silu(pre).astype(jnp.bfloat16)

        for i, (start, size) in enumerate(parts(c)):
            pl.when((start >= ext) | (l < layers - 1))(functools.partial(norm_part, i, start, size))
        ag_sent(l, c)
        stats(l, c).wait_send()
        nr_start(l, c)

    def do_hand(l, c):
        def go(k):
            nr_far(c, k).wait_recv()
            nr_forward(c, k).start()

        by_layer(c, l, go)

    def store_rows(c):
        r = pl.ds(c * CHUNK, CHUNK)
        return pltpu.make_async_copy(out_all.at[r, :], out_ref.at[r, :], out_sem.at[c])

    def do_half(l, c, q, final):
        for start, size in parts(c):
            if final and start < ext:
                continue
            r = slice(start, start + size)
            cols = pl.ds(pl.multiple_of(q * width, width), width)
            full = jnp.concatenate([nrm[b, r, :] for b in range(n_tp)], axis=1)
            branch = jnp.dot(full, wo_all[l, q], preferred_element_type=jnp.float32)
            new = (xf[tp, r, cols].astype(jnp.float32) + branch).astype(jnp.bfloat16)
            if final:
                out_all[start - ext:start - ext + size, cols] = new
            else:
                xf[tp, r, cols] = new

    def do_near(l, c, final):
        nr_wait(l, c)
        do_half(l, c, inner, final)

    def do_rest(l, c, final):
        do_half(l, c, PAIR - 1 - inner, final)
        if final:
            store_rows(c).start()
        else:
            ag_start(l + 1, c)
        nr_sent(l, c)

    by_head = near_end * (outer - tp) * (outer - tp) * (1 - (far_half - core) * (far_half - core)) == 1
    is_root = (near_end == 1) & (outer == tp)
    is_mid = (near_end == 1) & (outer != tp) & jnp.logical_not(by_head)
    is_head = (near_end == 0) & (outer == tp)
    is_end = (near_end == 0) & (outer != tp)

    roles = (
        (is_end, END_OPEN, END_PLAN), (is_head, HEAD_OPEN, HEAD_PLAN),
        (is_mid, MID_OPEN, MID_PLAN), (is_root, NEAR_OPEN, ROOT_PLAN), (by_head, NEAR_OPEN, NEXT_PLAN),
    )

    def act(kind, j, l, side):
        if kind == BEFORE:
            @pl.when(sp > 0)
            def _():
                before_copy().wait_recv()

            ag_start(0, 0)
        elif kind == SIDE:
            relay_side(j, l)
        elif kind == ZOWN:
            z_own(j, l)
        elif kind == XOWN:
            x_own(j, l).start()
        elif kind >= O:
            relay_o(l, j, kind)
        else:
            relay_piece(kind, l, j, side)

    for m in (V, G):
        z_own(m, 0)
        x_own(m, 0).start()
    @pl.when(sp < n_sp - 1)
    def _():
        before_copy().start()

    send_o(0)
    load_rows().wait()
    for c in range(1, n_chunks):
        ag_start(0, c)
    for l in range(1, layers):
        for m in range(PAIR):
            load_weight(m, l).wait()

    @pl.when(outer == tp)
    def _():
        for l in range(layers):
            load_out(l).wait()

    for small in smalls:
        small.wait()
    send_o(1)
    for role, order, _ in roles:
        @pl.when(role)
        def _():
            for kind, j, later in order:
                act(kind, j, later, False)

    for c in range(n_chunks):
        do_pass(0, c)
    w_ready(V, 0)
    w_ready(G, 0)

    def layer_body(l, carry):
        more = l < layers - 1

        def ahead(f):
            pl.when(more)(f)

        def slot(n):
            for role, _, plan in roles:
                for kind, j, later, *turn in plan.get(n, ()):
                    when = (role & (l + later < layers)) if later else role
                    for t in turn:
                        when = when & (l == 0, (l > 0) & (l < layers - 1), l > 0, l == layers - 2)[t]

                    @pl.when(when)
                    def _():
                        act(kind, j, l + later, True)

        def pass_next(c):
            ahead(lambda: do_pass(l + 1, c))

        do_glu(l, (0, 1))
        do_conv(l, 0)
        slot(1)
        do_conv(l, 1)
        do_glu(l, (2, 3))
        do_conv(l, 2)
        slot(2)
        do_norm(l, 0)
        do_conv(l, 3)
        do_norm(l, 1)
        slot(3)
        do_norm(l, 2)
        do_norm(l, 3)
        slot(4)
        @pl.when(more)
        def _():
            do_hand(l, 0)
            slot(5)
            do_hand(l, 1)
            slot(13)
            o_ready(l)
            do_near(l, 0, False)
            do_rest(l, 0, False)
            do_hand(l, 2)
            do_near(l, 1, False)
            do_rest(l, 1, False)
            slot(6)
            do_hand(l, 3)
            do_near(l, 2, False)
            do_rest(l, 2, False)
            slot(7)
            do_near(l, 3, False)
            do_rest(l, 3, False)

        @pl.when(l == layers - 1)
        def _():
            do_hand(l, 0)
            do_hand(l, 1)
            do_near(l, 0, True)
            do_hand(l, 2)
            do_near(l, 1, True)
            do_hand(l, 3)
            do_near(l, 2, True)
            do_near(l, 3, True)
            o_ready(l)
            for c in range(n_chunks):
                do_rest(l, c, True)

        @pl.when(l < layers - 2)
        def _():
            send_o(l + 2)

        slot(8)
        pass_next(0)
        slot(9)
        pass_next(1)
        slot(10)
        pass_next(2)
        slot(11)
        pass_next(3)
        slot(12)

        @pl.when(more)
        def _():
            w_ready(V, l + 1)
            w_ready(G, l + 1)

        return carry

    lax.fori_loop(0, layers, layer_body, 0)

    def sent(block, sem):
        remote(block, block, sem, before_r.at[0], x_peer, tp).wait_send()

    for m in range(PAIR):
        whole = (wv_all, wg_all)[m]
        sent(whole.at[:, pl.ds(0, n_out * depth), :], w_xsend.at[m])

        @pl.when(near_end == 0)
        def _():
            sent(whole.at[:, pl.ds(0, depth), :], w_zsend.at[m])

        @pl.when(near_end == 1)
        def _():
            sent(whole.at[:, pl.ds(0, (PAIR + last) * depth), :], w_zsend.at[m])

    @pl.when(outer != tp)
    def _():
        sent(wo_all.at[:, 0, pl.ds(0, chan), :], og_send.at[0])

    @pl.when(goes_up)
    def _():
        sent(wo_all.at[:, 0], o_send.at[0])

    @pl.when(goes_down)
    def _():
        sent(wo_all.at[:, 0], o_send.at[1])

    sent(wo_all.at[:, 0], o_send.at[2])

    @pl.when(sp < n_sp - 1)
    def _():
        before_copy().wait_send()

    for c in range(n_chunks):
        store_rows(c).wait()


def fused_shards(n_sp, n_tp, inputs, norm_gain, w_value, w_gate, conv_taps, ln_gain, ln_bias, w_out):
    layers, depth, chan = w_value.shape
    rows, dblk = inputs.shape
    width = w_out.shape[2]
    n_chunks = rows // CHUNK
    features = dblk * n_tp
    ext = HALO * layers
    bf16, f32 = jnp.bfloat16, jnp.float32
    dma = pltpu.SemaphoreType.DMA
    place = pl.BlockSpec(memory_space=pl.ANY)
    return pl.pallas_call(
        functools.partial(fused_kernel, n_sp, n_tp, 1e-06),
        out_shape=jax.ShapeDtypeStruct((rows, dblk), bf16),
        in_specs=[place] * 8,
        out_specs=place,
        scratch_shapes=[
            pltpu.VMEM(norm_gain.shape, f32),
            pltpu.VMEM(conv_taps.shape, f32),
            pltpu.VMEM(ln_gain.shape, f32),
            pltpu.VMEM(ln_bias.shape, f32),
            pltpu.VMEM((rows, dblk), bf16),
            pltpu.VMEM((layers, n_sp * depth, chan), bf16),
            pltpu.VMEM((layers, n_sp * depth, chan), bf16),
            pltpu.VMEM((layers, PAIR, n_tp * chan, width), bf16),
            pltpu.VMEM((n_tp, ext + rows, dblk), bf16),
            pltpu.VMEM((ext + PAIR * CHUNK, features), bf16),
            pltpu.VMEM((chan // LANES, HALO + ext + rows, LANES), f32),
            pltpu.VMEM((ext + rows, chan), f32),
            pltpu.VMEM((layers, n_chunks, n_tp, 16, CHUNK), f32),
            pltpu.VMEM((n_tp, ext + rows, chan), bf16),
            dma((layers, PAIR, n_sp // PAIR)),
            dma((layers, PAIR, 2)),
            dma((PAIR,)),
            dma((PAIR,)),
            dma((layers, n_tp)),
            dma((layers,)),
            dma((3,)),
            dma((1,)),
            dma((2, n_chunks)),
            dma((n_chunks,)),
            dma((1,)),
            dma((1,)),
            dma((n_chunks,)),
            dma((n_chunks,)),
            dma((2, n_chunks)),
            dma((n_chunks,)),
            dma((3, layers)),
            dma((5,)),
            dma((n_chunks,)),
        ],
        compiler_params=pltpu.CompilerParams(collective_id=0, has_side_effects=True),
    )(
        inputs,
        norm_gain,
        w_value,
        w_gate,
        conv_taps,
        ln_gain,
        ln_bias,
        w_out,
    )


def fits_kernel(n_sp, n_tp, inputs, w_value, conv_taps, w_out):
    rows, dblk = inputs.shape
    width = w_out.shape[2]
    return (
        n_sp == 4 * PAIR
        and n_tp == PAIR * PAIR
        and rows % CHUNK == 0
        and rows // CHUNK >= 4
        and w_value.shape[0] >= 2
        and w_value.shape[1] % LANES == 0
        and w_value.shape[2] % LANES == 0
        and width % LANES == 0
        and dblk == PAIR * width
        and conv_taps.shape[1] - 1 <= HALO
        and HALO * w_value.shape[0] <= CHUNK
        and rows // CHUNK == 4
    )


def shards(inputs, norm_gain, w_value, w_gate, conv_taps, ln_gain, ln_bias, w_out):
    n_sp, n_tp = lax.axis_size("sp"), lax.axis_size("tp")
    args = (inputs, norm_gain, w_value, w_gate, conv_taps, ln_gain, ln_bias, w_out)
    if fits_kernel(n_sp, n_tp, inputs, w_value, conv_taps, w_out):
        return fused_shards(n_sp, n_tp, *args)
    return plain_shards(*args)


def from_behind(block, axis, distance):
    devices = range(lax.axis_size(axis))
    route = [(i - distance, i) for i in devices if i - distance in devices]
    return lax.ppermute(block, axis, route)


def plain_shards(inputs, norm_gain, w_value, w_gate, conv_taps, ln_gain, ln_bias, w_out):
    rows = inputs.shape[0]
    reach = conv_taps.shape[1] - 1
    layers = conv_taps.shape[0]
    channels = conv_taps.shape[2] * lax.axis_size("tp")
    whole_value, whole_gate, whole_out = (
        lax.all_gather(w_value, "sp", axis=1, tiled=True),
        lax.all_gather(w_gate, "sp", axis=1, tiled=True),
        lax.all_gather(w_out, "sp", axis=2, tiled=True),
    )
    stream = inputs
    for layer in range(layers):
        full_rows = lax.all_gather(stream, "tp", axis=1, tiled=True)
        xf = full_rows.astype(jnp.float32)
        meansq = jnp.mean(xf * xf, axis=1, keepdims=True)
        hidden = (xf * lax.rsqrt(meansq + 1e-06) * norm_gain[layer][None, :]).astype(jnp.bfloat16)
        value = jnp.dot(hidden, whole_value[layer], preferred_element_type=jnp.float32)
        gate = jnp.dot(hidden, whole_gate[layer], preferred_element_type=jnp.float32)
        glu = (value * jax.nn.sigmoid(gate)).astype(jnp.bfloat16)
        rim = from_behind(glu[rows - reach :], "sp", 1)
        padded = jnp.concatenate([rim, glu], axis=0)
        count = padded.shape[0] - reach
        filtered = jnp.zeros((count, glu.shape[1]), jnp.float32)
        for tap in range(reach + 1):
            filtered = filtered + conv_taps[layer, tap][None, :] * padded[tap : tap + count].astype(
                jnp.float32
            )
        total_sum, total_sq = lax.psum(
            (jnp.sum(filtered, axis=1), jnp.sum(filtered * filtered, axis=1)), "tp"
        )
        mean_val = (total_sum / channels)[:, None]
        var_val = (total_sq / channels)[:, None] - mean_val * mean_val
        normed = jax.nn.silu(
            (filtered - mean_val) * lax.rsqrt(var_val + 1e-06) * ln_gain[layer][None, :]
            + ln_bias[layer][None, :]
        ).astype(jnp.bfloat16)
        partial_out = jnp.dot(normed, whole_out[layer], preferred_element_type=jnp.float32)
        summed = lax.psum_scatter(
            partial_out.astype(jnp.bfloat16), "tp", scatter_dimension=1, tiled=True
        ).astype(jnp.float32)
        kept = stream.astype(jnp.float32)
        stream = (kept + summed).astype(jnp.bfloat16)
    return stream


def solution(mesh):
    in_specs = (
        P("sp", "tp"),
        P(),
        P(None, "sp", "tp"),
        P(None, "sp", "tp"),
        P(None, None, "tp"),
        P(None, "tp"),
        P(None, "tp"),
        P(None, "tp", "sp"),
    )
    out_specs = P("sp", "tp")
    return jax.shard_map(shards, mesh=mesh, in_specs=in_specs, out_specs=out_specs, check_vma=False)
```

```python
import functools

import jax
import jax.numpy as jnp
from jax import lax
from jax.experimental import pallas as pl
from jax.experimental.pallas import tpu as pltpu
from jax.sharding import PartitionSpec as P

MESH = pl.DeviceIdType.MESH
PAIR = 2
CHUNK = 128
HALO = 32
LANES = 128
V, G, O, UP, OVER, ZOWN, XOWN, BEFORE, SIDE = 0, 1, 2, 3, 4, 5, 6, 7, 8
OWN_X = ((XOWN, V, 1), (XOWN, G, 1))
OWN_Z = ((ZOWN, V, 1), (ZOWN, G, 1))
FIRST, EARLY, RISEN, LAST = 0, 1, 2, 3
LAST_X = ((XOWN, V, 2), (XOWN, G, 2))
LAST_Z = ((ZOWN, V, 2), (ZOWN, G, 2))


def every(kind, later):
    return tuple((kind, j, later) for j in range(4))


END_OPEN = (
    (V, 0, 0), *OWN_Z, (G, 0, 0), (V, 1, 0), (BEFORE, 0, 0), (G, 1, 0), (V, 2, 0), (G, 2, 0), (O, 0, 0),
    (XOWN, V, 1),
)
HEAD_OPEN = (
    (V, 0, 0), *every(UP, 0), *OWN_Z, (G, 0, 0), (V, 1, 0), (BEFORE, 0, 0), (G, 1, 0), (V, 2, 0), (G, 2, 0),
    *every(OVER, 0), *OWN_X,
)
MID_OPEN = (
    (V, 0, 0), (V, 1, 0), (G, 0, 0), (G, 1, 0), (V, 2, 0), (BEFORE, 0, 0), (G, 2, 0),
    (O, 0, 0), (O, 1, 0), (ZOWN, V, 1), (O, 2, 0),
)
NEAR_OPEN = (
    (V, 0, 0), (V, 1, 0), (G, 0, 0), (G, 1, 0), (V, 2, 0), (BEFORE, 0, 0), (G, 2, 0),
    *every(O, 0), *OWN_Z, *OWN_X,
)
SOON_OPEN = (*END_OPEN, (O, 1, 0))
SOON_PLAN = {
    1: ((O, 1, 0, RISEN), (O, 2, 0)), 2: ((O, 3, 0),), 3: ((XOWN, V, 1, RISEN), (XOWN, G, 1)), 4: ((V, 0, 1), *LAST_Z),
    13: ((G, 0, 1, FIRST), (V, 1, 1, FIRST), (V, 2, 1, FIRST)),
    6: ((V, 1, 1, RISEN),), 7: ((V, 2, 1, RISEN), (SIDE, V, 1)), 8: ((G, 0, 1, RISEN), (SIDE, G, 1)),
    9: ((G, 1, 1),), 10: ((G, 2, 1),), 12: ((O, 0, 1),),
}
END_PLAN = {
    1: ((O, 0, 0, RISEN), (O, 1, 0, EARLY)), 2: ((O, 2, 0, EARLY), (O, 1, 0, LAST)),
    3: ((O, 3, 0, EARLY), (XOWN, G, 1), (O, 2, 0, LAST)), 4: ((V, 0, 1), *LAST_Z, (O, 3, 0, LAST)),
    13: ((G, 0, 1, FIRST), (V, 1, 1, FIRST), (V, 2, 1, FIRST)),
    6: ((V, 1, 1, RISEN),), 7: ((V, 2, 1, RISEN), (SIDE, V, 1)), 8: ((G, 0, 1, RISEN), (SIDE, G, 1)),
    9: ((G, 1, 1),), 10: ((G, 2, 1),), 12: ((XOWN, V, 2),),
}
HEAD_PLAN = {
    3: every(UP, 1), 5: ((V, 0, 1), *LAST_Z), 6: ((V, 1, 1),), 7: ((V, 2, 1), (SIDE, V, 1)),
    8: ((G, 0, 1), (SIDE, G, 1)), 9: ((G, 1, 1),), 10: ((G, 2, 1), *every(OVER, 1), *LAST_X),
}
MID_PLAN = {
    1: ((O, 3, 0, FIRST), (ZOWN, G, 1), *OWN_X), 2: ((V, 0, 1), (V, 1, 1)), 3: ((V, 2, 1),), 4: ((G, 0, 1), (SIDE, V, 1)),
    5: ((G, 1, 1),), 6: ((G, 2, 1),), 7: ((SIDE, G, 1),),
    9: ((O, 0, 1),), 10: ((O, 1, 1),), 11: ((O, 2, 1),), 12: ((O, 3, 1), (ZOWN, V, 2)),
}
ROOT_PLAN = {
    1: ((V, 0, 1),), 2: ((V, 1, 1),), 3: ((V, 2, 1),), 4: ((G, 0, 1),), 5: ((G, 1, 1), (SIDE, V, 1)),
    6: ((G, 2, 1),), 7: ((SIDE, G, 1), (O, 0, 1), (O, 1, 1)), 8: ((O, 2, 1), (O, 3, 1), *LAST_Z, *LAST_X),
}
NEXT_PLAN = {
    1: ((V, 0, 1),), 2: ((V, 1, 1),), 3: ((V, 2, 1),), 4: ((G, 0, 1), (UP, 0, 1)), 5: ((G, 1, 1), (UP, 1, 1), (SIDE, V, 1)),
    6: ((G, 2, 1), (UP, 2, 1)), 7: ((SIDE, G, 1), (UP, 3, 1)),
    8: (*every(OVER, 1), *LAST_Z, *LAST_X),
}


def fused_kernel(
    n_sp, n_tp, eps,
    x_ref, gain_hbm, wv_ref, wg_ref, taps_hbm, lng_hbm, lnb_hbm, wo_ref,
    out_ref,
    gain_ref, taps_ref, lng_ref, lnb_ref, out_all, wv_all, wg_all, wo_all, xf, hid, glu, filt, stat, nrm,
    w_recv, w_xrecv, w_zsend, w_xsend, o_recv, o_xrecv, o_send, og_send,
    ag_recv, ag_send, before_s, before_r, st_recv, st_send, nr_recv, nr_send,
    in_sem, small_sem, out_sem,
):
    sp = lax.axis_index("sp")
    tp = lax.axis_index("tp")
    layers, depth = wv_ref.shape[0], wv_ref.shape[1]
    rows, dblk = x_ref.shape
    width = wo_ref.shape[2]
    chan = wv_ref.shape[2]
    taps = taps_ref.shape[1]
    features = dblk * n_tp
    channels = chan * n_tp
    n_chunks = rows // CHUNK
    n_out = n_sp // PAIR
    outer, inner = lax.div(sp, PAIR), lax.rem(sp, PAIR)
    x_peer = outer * PAIR + (PAIR - 1 - inner)
    far_half, core = lax.div(tp, PAIR), lax.rem(tp, PAIR)
    partner = far_half * PAIR + (PAIR - 1 - core)
    far = (n_tp // PAIR - 1 - far_half) * PAIR + core
    first_off = HALO - (taps - 1)
    ext = HALO * layers
    halves = chan // LANES

    last = n_out - 1
    upper = lax.div(outer, n_out // 2)
    near_end = outer + upper * (last - 2 * outer)

    def line(j):
        near = j + 1 - (near_end if j == 0 else 0)
        return near + upper * (last - 2 * near)

    slant = sp + 2 * inner - 1
    has_slant = (slant >= 0) & (slant < n_sp)
    barrier = pltpu.get_barrier_semaphore()

    def greet(sp_to, tp_to):
        pl.semaphore_signal(barrier, inc=1, device_id=(sp_to, tp_to), device_id_type=MESH)

    greet(line(0) * PAIR + inner, tp)
    greet(x_peer, tp)
    for step in range(1, n_tp):
        greet(sp, lax.rem(tp + step, n_tp))

    @pl.when(near_end == 1)
    def _():
        greet(line(1) * PAIR + inner, tp)

    @pl.when(has_slant)
    def _():
        greet(slant, tp)

    def own_rows(s):
        return pl.ds(pl.multiple_of(s * depth, depth), depth)

    def o_slot(l, x, b):
        return wo_all.at[l, x, pl.ds(pl.multiple_of(b * chan, chan), chan), :]

    def load_weight(m, l):
        src, dst = ((wv_ref, wv_all), (wg_ref, wg_all))[m]
        return pltpu.make_async_copy(src.at[l], dst.at[l, own_rows(sp), :], in_sem.at[m, l])

    def load_out(l):
        return pltpu.make_async_copy(wo_ref.at[l], o_slot(l, inner, tp), in_sem.at[2, l])

    def load_rows():
        return pltpu.make_async_copy(x_ref, xf.at[tp, pl.ds(ext, rows), :], small_sem.at[4])

    smalls = [
        pltpu.make_async_copy(src, dst, small_sem.at[i])
        for i, (src, dst) in enumerate(
            ((gain_hbm, gain_ref), (taps_hbm, taps_ref), (lng_hbm, lng_ref), (lnb_hbm, lnb_ref)))
    ]
    for m in range(PAIR):
        load_weight(m, 0).start()
    load_rows().start()

    @pl.when(outer == tp)
    def _():
        for l in range(layers):
            load_out(l).start()

    for l in range(1, layers):
        for m in range(PAIR):
            load_weight(m, l).start()
    for small in smalls:
        small.start()

    glu[:, 0:HALO, :] = jnp.zeros((halves, HALO, LANES), jnp.float32)

    @pl.when(sp == 0)
    def _():
        xf[tp, 0:ext, :] = jnp.zeros((ext, dblk), jnp.bfloat16)


    for m in range(PAIR):
        load_weight(m, 0).wait()
    pl.semaphore_wait(barrier, 2 + n_tp - 1 + near_end + has_slant.astype(jnp.int32))

    def parts(c):
        own = (ext + c * CHUNK, CHUNK)
        return ((0, ext), own) if c == 0 else (own,)

    def chunk_rows(c, skip):
        return pl.ds(ext + c * CHUNK, CHUNK) if c else pl.ds(skip * HALO, ext - skip * HALO + CHUNK)

    def by_layer(c, l, f):
        if c or isinstance(l, int):
            f(0 if c else l)
        else:
            for k in range(layers):
                pl.when(l == k)(functools.partial(f, k))

    def stat_rows(c):
        return pl.ds(0, 8 * len(parts(c)))

    def remote(src, dst, send, recv, sp_to, tp_to):
        return pltpu.make_async_remote_copy(
            src_ref=src, dst_ref=dst, send_sem=send, recv_sem=recv,
            device_id=(sp_to, tp_to), device_id_type=MESH,
        )

    def w_slot(m, l, s):
        return (wv_all, wg_all)[m].at[l, own_rows(s), :]

    def z_copy(m, l, j):
        to = line(j) * PAIR + inner
        return remote(w_slot(m, l, sp), w_slot(m, l, sp), w_zsend.at[m], w_recv.at[l, m, outer], to, tp)

    def z_arrival(m, l, j):
        s = line(j) * PAIR + inner
        return remote(w_slot(m, l, s), w_slot(m, l, s), w_zsend.at[m], w_recv.at[l, m, line(j)], s, tp)

    def z_forward(m, l, j):
        s = line(j) * PAIR + inner
        to = line(1 if j == 0 else 0) * PAIR + inner
        slot = w_slot(m, l, s)
        return remote(slot, slot, w_zsend.at[m], w_recv.at[l, m, line(j)], to, tp)

    def x_own(m, l):
        return remote(w_slot(m, l, sp), w_slot(m, l, sp), w_xsend.at[m], w_xrecv.at[l, m, 0], x_peer, tp)

    def x_copy(m, l, j):
        s = line(j) * PAIR + inner
        slot = w_slot(m, l, s)
        return remote(slot, slot, w_xsend.at[m], w_xrecv.at[l, m, 1], x_peer, tp)

    def x_arrival(m, l):
        slot = w_slot(m, l, x_peer)
        return remote(slot, slot, w_xsend.at[m], w_xrecv.at[l, m, 0], x_peer, tp)

    def x_arrivals(m, l):
        block = (wv_all, wg_all)[m].at[l, pl.ds(0, last * depth), :]
        return remote(block, block, w_xsend.at[m], w_xrecv.at[l, m, 1], x_peer, tp)

    def side_copy(m, l):
        to = line(0) * PAIR + inner
        slot = w_slot(m, l, x_peer)
        return remote(slot, slot, w_xsend.at[m], w_xrecv.at[l, m, 1], to, tp)

    def z_own(m, l):
        z_copy(m, l, 0).start()

        @pl.when(near_end == 1)
        def _():
            z_copy(m, l, 1).start()

    def relay_piece(m, l, j, side):
        z_arrival(m, l, j).wait_recv()

        @pl.when(near_end == 1)
        def _():
            z_forward(m, l, j).start()

        if j or not side:
            x_copy(m, l, j).start()
        elif m == V:
            @pl.when(jnp.logical_not(by_side(m, l)))
            def _():
                x_copy(m, l, j).start()

    def by_side(m, l):
        return l > 0 if m == G else (l > 0) & ((l < layers - 1) | (upper == far_half))

    def relay_side(m, l):
        @pl.when(by_side(m, l))
        def _():
            x_arrival(m, l).wait_recv()
            side_copy(m, l).start()

    def w_ready(m, l):
        @pl.when(jnp.logical_not(by_side(m, l)))
        def _():
            x_arrival(m, l).wait_recv()

        x_arrivals(m, l).wait_recv()

    def o_gather(l):
        return remote(wo_ref.at[l], o_slot(l, inner, tp), og_send.at[0], o_recv.at[l, tp], sp, outer)

    def o_hop(l, j, way, to):
        b = lax.rem(tp + j, n_tp)
        slot = o_slot(l, inner, b)
        return remote(slot, slot, o_send.at[way], o_xrecv.at[l] if way == 2 else o_recv.at[l, b], to, tp)

    def o_arrival(l, b):
        slot = o_slot(l, inner, b)
        return remote(slot, slot, o_send.at[0], o_recv.at[l, b], x_peer, tp)

    goes_up = (outer >= tp) & (outer < last)
    goes_down = (outer <= tp) & (outer > 0)

    def send_o(l):
        @pl.when(outer != tp)
        def _():
            o_gather(l).start()

    def o_arrived(l, j):
        if j == 0:
            @pl.when(outer != tp)
            def _():
                o_arrival(l, tp).wait_recv()
        else:
            o_arrival(l, lax.rem(tp + j, n_tp)).wait_recv()

    def o_along(l, j):
        @pl.when(goes_up)
        def _():
            o_hop(l, j, 0, sp + PAIR).start()

        @pl.when(goes_down)
        def _():
            o_hop(l, j, 1, sp - PAIR).start()

    def relay_o(l, j, kind):
        if kind != OVER:
            o_arrived(l, j)
            o_along(l, j)
        if kind != UP:
            o_hop(l, j, 2, x_peer).start()

    def o_ready(l):
        block = wo_all.at[l, 0]
        remote(block, block, o_send.at[2], o_xrecv.at[l], x_peer, tp).wait_recv()

    def ag_far(c, l):
        r = chunk_rows(c, l)
        return remote(xf.at[tp, r, :], xf.at[tp, r, :], ag_send.at[c], ag_recv.at[0, c], sp, far)

    def ag_partner(c, l):
        r = chunk_rows(c, l)
        return remote(xf.at[tp, r, :], xf.at[tp, r, :], ag_send.at[c], ag_recv.at[1, c], sp, partner)

    def ag_forward(c, l):
        r = chunk_rows(c, l)
        return remote(xf.at[far, r, :], xf.at[far, r, :], ag_send.at[c], ag_recv.at[1, c], sp, partner)

    def nr_far(c, l):
        r = chunk_rows(c, l + 1)
        return remote(nrm.at[tp, r, :], nrm.at[tp, r, :], nr_send.at[c], nr_recv.at[0, c], sp, far)

    def nr_partner(c, l):
        r = chunk_rows(c, l + 1)
        return remote(nrm.at[tp, r, :], nrm.at[tp, r, :], nr_send.at[c], nr_recv.at[1, c], sp, partner)

    def nr_forward(c, l):
        r = chunk_rows(c, l + 1)
        return remote(nrm.at[far, r, :], nrm.at[far, r, :], nr_send.at[c], nr_recv.at[1, c], sp, partner)

    def stat_copy(l, c, step):
        to = lax.rem(tp + step, n_tp)
        return remote(stat.at[l, c, tp, stat_rows(c), :], stat.at[l, c, tp, stat_rows(c), :], st_send.at[c], st_recv.at[c], sp, to)

    def stats(l, c):
        block = stat.at[l, c, pl.ds(0, n_tp - 1), stat_rows(c), :]
        return remote(block, block, st_send.at[c], st_recv.at[c], sp, far)

    def before_copy():
        to = lax.rem(sp + 1, n_sp)
        return remote(x_ref.at[pl.ds(rows - ext, ext), :], xf.at[tp, pl.ds(0, ext), :], before_s.at[0], before_r.at[0], to, tp)

    def do_pass(l, c):
        def go(k):
            ag_far(c, k).wait_recv()
            ag_forward(c, k).start()

        by_layer(c, l, go)

    def ag_start(l, c):
        def go(k):
            ag_far(c, k).start()
            ag_partner(c, k).start()

        by_layer(c, l, go)

    def ag_sent(l, c):
        def go(k):
            block = xf.at[pl.ds(0, 3), chunk_rows(c, k), :]
            remote(block, block, ag_send.at[c], ag_recv.at[1, c], sp, far).wait_send()

        by_layer(c, l, go)

    def ag_wait(l, c):
        def go(k):
            block = xf.at[pl.ds(0, PAIR), chunk_rows(c, k), :]
            remote(block, block, ag_send.at[c], ag_recv.at[1, c], sp, partner).wait_recv()

        by_layer(c, l, go)

    def nr_start(l, c):
        def go(k):
            nr_far(c, k).start()
            nr_partner(c, k).start()

        by_layer(c, l, go)

    def nr_sent(l, c):
        def go(k):
            block = nrm.at[pl.ds(0, 3), chunk_rows(c, k + 1), :]
            remote(block, block, nr_send.at[c], nr_recv.at[1, c], sp, far).wait_send()

        by_layer(c, l, go)

    def nr_wait(l, c):
        def go(k):
            block = nrm.at[pl.ds(0, PAIR), chunk_rows(c, k + 1), :]
            remote(block, block, nr_send.at[c], nr_recv.at[1, c], sp, partner).wait_recv()

        by_layer(c, l, go)

    def do_glu(l, cs):
        for c in cs:
            ag_wait(l, c)

        def glu_part(start, size):
            r = slice(start, start + size)
            blocks = [xf[b, r, :].astype(jnp.float32) for b in range(n_tp)]
            total = sum(jnp.sum(b * b, axis=1, keepdims=True) for b in blocks)
            scale = lax.rsqrt(total / features + eps)
            for b in range(n_tp):
                cols = slice(b * dblk, (b + 1) * dblk)
                hid[0:size, cols] = (
                    xf[b, r, :].astype(jnp.float32) * scale * gain_ref[pl.ds(l, 1), cols]).astype(jnp.bfloat16)
            h = hid[0:size, :]
            value = jnp.dot(h, wv_all[l], preferred_element_type=jnp.float32)
            gate = jnp.dot(h, wg_all[l], preferred_element_type=jnp.float32)
            g = (value * jax.nn.sigmoid(gate)).astype(jnp.bfloat16).astype(jnp.float32)
            if start < ext:
                row = lax.broadcasted_iota(jnp.int32, g.shape, 0)
                g = jnp.where((row >= ext - start) | (sp > 0), g, 0.0)
            for k in range(halves):
                glu[k, HALO + start:HALO + start + size, :] = g[:, k * LANES:(k + 1) * LANES]

        start, size = ext + cs[0] * CHUNK, len(cs) * CHUNK
        if cs[0]:
            glu_part(start, size)
        else:
            pl.when(l < layers - 1)(functools.partial(glu_part, 0, start + size))
            pl.when(l == layers - 1)(functools.partial(glu_part, ext - HALO, HALO + size))

    def do_conv(l, c):
        def conv_part(i, start, size):
            sums = jnp.zeros((size, 1), jnp.float32)
            squares = jnp.zeros((size, 1), jnp.float32)
            for k in range(halves):
                acc = jnp.zeros((size, LANES), jnp.float32)
                for tap in range(taps):
                    acc = acc + taps_ref[l, tap:tap + 1, k * LANES:(k + 1) * LANES] * glu[
                        k, start + first_off + tap:start + first_off + tap + size, :]
                filt[start:start + size, k * LANES:(k + 1) * LANES] = acc
                sums = sums + jnp.sum(acc, axis=1, keepdims=True)
                squares = squares + jnp.sum(acc * acc, axis=1, keepdims=True)
            lane = lax.broadcasted_iota(jnp.int32, (size, LANES), 1)
            both = jnp.where(lane == 0, sums, squares)
            if size < CHUNK:
                both = jnp.concatenate([both, jnp.zeros((CHUNK - size, LANES), jnp.float32)], axis=0)
            stat[l, c, tp, 8 * i:8 * i + 8, :] = jnp.transpose(both)[0:8, :]

        for i, (start, size) in enumerate(parts(c)):
            if start < ext:
                pl.when(l < layers - 1)(functools.partial(conv_part, i, start, size))
            else:
                conv_part(i, start, size)
        for step in range(1, n_tp):
            stat_copy(l, c, step).start()

    def do_norm(l, c):
        stats(l, c).wait_recv()

        def norm_part(i, start, size):
            r = slice(start, start + size)
            tot = stat[l, c, 0, 8 * i:8 * i + 8, :]
            for b in range(1, n_tp):
                tot = tot + stat[l, c, b, 8 * i:8 * i + 8, :]
            tot = jnp.transpose(jnp.concatenate([tot, jnp.zeros((LANES - 8, CHUNK), jnp.float32)], axis=0))
            mean = tot[0:size, 0:1] / channels
            var = tot[0:size, 1:2] / channels - mean * mean
            pre = (filt[r, :] - mean) * lax.rsqrt(var + eps) * lng_ref[pl.ds(l, 1), :] + lnb_ref[pl.ds(l, 1), :]
            nrm[tp, r, :] = jax.nn.silu(pre).astype(jnp.bfloat16)

        for i, (start, size) in enumerate(parts(c)):
            pl.when((start >= ext) | (l < layers - 1))(functools.partial(norm_part, i, start, size))
        ag_sent(l, c)
        stats(l, c).wait_send()
        nr_start(l, c)

    def do_hand(l, c):
        def go(k):
            nr_far(c, k).wait_recv()
            nr_forward(c, k).start()

        by_layer(c, l, go)

    def store_rows(c):
        r = pl.ds(c * CHUNK, CHUNK)
        return pltpu.make_async_copy(out_all.at[r, :], out_ref.at[r, :], out_sem.at[c])

    def do_half(l, c, q, final):
        for start, size in parts(c):
            if final and start < ext:
                continue
            r = slice(start, start + size)
            cols = pl.ds(pl.multiple_of(q * width, width), width)
            full = jnp.concatenate([nrm[b, r, :] for b in range(n_tp)], axis=1)
            branch = jnp.dot(full, wo_all[l, q], preferred_element_type=jnp.float32)
            new = (xf[tp, r, cols].astype(jnp.float32) + branch).astype(jnp.bfloat16)
            if final:
                out_all[start - ext:start - ext + size, cols] = new
            else:
                xf[tp, r, cols] = new

    def do_near(l, c, final):
        nr_wait(l, c)
        do_half(l, c, inner, final)

    def do_rest(l, c):
        do_half(l, c, PAIR - 1 - inner, False)
        ag_start(l + 1, c)
        nr_sent(l, c)

    by_head = near_end * (outer - tp) * (outer - tp) * (1 - (far_half - core) * (far_half - core)) == 1
    is_root = (near_end == 1) & (outer == tp)
    is_mid = (near_end == 1) & (outer != tp) & jnp.logical_not(by_head)
    is_head = (near_end == 0) & (outer == tp)
    is_soon = (near_end == 0) & ((outer - tp) * (outer - tp) == 1)
    is_end = (near_end == 0) & ((outer - tp) * (outer - tp) > 1)

    roles = (
        (is_end, END_OPEN, END_PLAN), (is_soon, SOON_OPEN, SOON_PLAN), (is_head, HEAD_OPEN, HEAD_PLAN),
        (is_mid, MID_OPEN, MID_PLAN), (is_root, NEAR_OPEN, ROOT_PLAN), (by_head, NEAR_OPEN, NEXT_PLAN),
    )

    def act(kind, j, l, side):
        if kind == BEFORE:
            @pl.when(sp > 0)
            def _():
                before_copy().wait_recv()

            ag_start(0, 0)
        elif kind == SIDE:
            relay_side(j, l)
        elif kind == ZOWN:
            z_own(j, l)
        elif kind == XOWN:
            x_own(j, l).start()
        elif kind >= O:
            relay_o(l, j, kind)
        else:
            relay_piece(kind, l, j, side)

    for m in (V, G):
        z_own(m, 0)
        x_own(m, 0).start()
    @pl.when(sp < n_sp - 1)
    def _():
        before_copy().start()

    send_o(0)
    load_rows().wait()
    for c in range(1, n_chunks):
        ag_start(0, c)
    for l in range(1, layers):
        for m in range(PAIR):
            load_weight(m, l).wait()

    @pl.when(outer == tp)
    def _():
        for l in range(layers):
            load_out(l).wait()

    for small in smalls:
        small.wait()
    send_o(1)
    for role, order, _ in roles:
        @pl.when(role)
        def _():
            for kind, j, later in order:
                act(kind, j, later, False)

    for c in range(n_chunks):
        do_pass(0, c)
    w_ready(V, 0)
    w_ready(G, 0)

    def layer_body(l, carry):
        more = l < layers - 1

        def ahead(f):
            pl.when(more)(f)

        def slot(n):
            for role, _, plan in roles:
                for kind, j, later, *turn in plan.get(n, ()):
                    when = (role & (l + later < layers)) if later else role
                    for t in turn:
                        when = when & (l == 0, l < layers - 1, l > 0, l == layers - 1)[t]

                    @pl.when(when)
                    def _():
                        act(kind, j, l + later, True)

        def pass_next(c):
            ahead(lambda: do_pass(l + 1, c))

        do_glu(l, (0,))
        do_conv(l, 0)
        slot(1)
        do_glu(l, (1,))
        do_conv(l, 1)
        do_glu(l, (2, 3))
        do_conv(l, 2)
        slot(2)
        do_norm(l, 0)
        do_conv(l, 3)
        do_norm(l, 1)
        slot(3)
        do_norm(l, 2)
        do_norm(l, 3)
        slot(4)
        @pl.when(more)
        def _():
            do_hand(l, 0)
            slot(5)
            do_hand(l, 1)
            slot(13)
            o_ready(l)
            do_near(l, 0, False)
            do_rest(l, 0)
            do_hand(l, 2)
            do_near(l, 1, False)
            do_rest(l, 1)
            slot(6)
            do_hand(l, 3)
            do_near(l, 2, False)
            do_rest(l, 2)
            slot(7)
            do_near(l, 3, False)
            do_rest(l, 3)

        @pl.when(l == layers - 1)
        def _():
            do_hand(l, 0)
            do_hand(l, 1)
            do_near(l, 0, True)
            do_hand(l, 2)
            do_near(l, 1, True)
            do_hand(l, 3)
            do_near(l, 2, True)
            do_near(l, 3, True)
            o_ready(l)
            for c in range(0, n_chunks, PAIR):
                r = slice(c * CHUNK, (c + PAIR) * CHUNK)
                q = PAIR - 1 - inner
                cols = pl.ds(pl.multiple_of(q * width, width), width)
                x_rows = slice(ext + c * CHUNK, ext + (c + PAIR) * CHUNK)
                full = jnp.concatenate([nrm[b, x_rows, :] for b in range(n_tp)], axis=1)
                branch = jnp.dot(full, wo_all[l, q], preferred_element_type=jnp.float32)
                out_all[r, cols] = (xf[tp, x_rows, cols].astype(jnp.float32) + branch).astype(jnp.bfloat16)
                for k in range(c, c + PAIR):
                    store_rows(k).start()
            for c in range(n_chunks):
                nr_sent(l, c)

        @pl.when(l < layers - 2)
        def _():
            send_o(l + 2)

        slot(8)
        pass_next(0)
        slot(9)
        pass_next(1)
        slot(10)
        pass_next(2)
        slot(11)
        pass_next(3)
        slot(12)

        @pl.when(more)
        def _():
            w_ready(V, l + 1)
            w_ready(G, l + 1)

        return carry

    lax.fori_loop(0, layers, layer_body, 0)

    def sent(block, sem):
        remote(block, block, sem, before_r.at[0], x_peer, tp).wait_send()

    for m in range(PAIR):
        whole = (wv_all, wg_all)[m]
        sent(whole.at[:, pl.ds(0, n_out * depth), :], w_xsend.at[m])

        @pl.when(near_end == 0)
        def _():
            sent(whole.at[:, pl.ds(0, depth), :], w_zsend.at[m])

        @pl.when(near_end == 1)
        def _():
            sent(whole.at[:, pl.ds(0, (PAIR + last) * depth), :], w_zsend.at[m])

    @pl.when(outer != tp)
    def _():
        sent(wo_all.at[:, 0, pl.ds(0, chan), :], og_send.at[0])

    @pl.when(goes_up)
    def _():
        sent(wo_all.at[:, 0], o_send.at[0])

    @pl.when(goes_down)
    def _():
        sent(wo_all.at[:, 0], o_send.at[1])

    sent(wo_all.at[:, 0], o_send.at[2])

    @pl.when(sp < n_sp - 1)
    def _():
        before_copy().wait_send()

    for c in range(n_chunks):
        store_rows(c).wait()


def fused_shards(n_sp, n_tp, inputs, norm_gain, w_value, w_gate, conv_taps, ln_gain, ln_bias, w_out):
    layers, depth, chan = w_value.shape
    rows, dblk = inputs.shape
    width = w_out.shape[2]
    n_chunks = rows // CHUNK
    features = dblk * n_tp
    ext = HALO * layers
    bf16, f32 = jnp.bfloat16, jnp.float32
    dma = pltpu.SemaphoreType.DMA
    place = pl.BlockSpec(memory_space=pl.ANY)
    return pl.pallas_call(
        functools.partial(fused_kernel, n_sp, n_tp, 1e-06),
        out_shape=jax.ShapeDtypeStruct((rows, dblk), bf16),
        in_specs=[place] * 8,
        out_specs=place,
        scratch_shapes=[
            pltpu.VMEM(norm_gain.shape, f32),
            pltpu.VMEM(conv_taps.shape, f32),
            pltpu.VMEM(ln_gain.shape, f32),
            pltpu.VMEM(ln_bias.shape, f32),
            pltpu.VMEM((rows, dblk), bf16),
            pltpu.VMEM((layers, n_sp * depth, chan), bf16),
            pltpu.VMEM((layers, n_sp * depth, chan), bf16),
            pltpu.VMEM((layers, PAIR, n_tp * chan, width), bf16),
            pltpu.VMEM((n_tp, ext + rows, dblk), bf16),
            pltpu.VMEM((ext + PAIR * CHUNK, features), bf16),
            pltpu.VMEM((chan // LANES, HALO + ext + rows, LANES), f32),
            pltpu.VMEM((ext + rows, chan), f32),
            pltpu.VMEM((layers, n_chunks, n_tp, 16, CHUNK), f32),
            pltpu.VMEM((n_tp, ext + rows, chan), bf16),
            dma((layers, PAIR, n_sp // PAIR)),
            dma((layers, PAIR, 2)),
            dma((PAIR,)),
            dma((PAIR,)),
            dma((layers, n_tp)),
            dma((layers,)),
            dma((3,)),
            dma((1,)),
            dma((2, n_chunks)),
            dma((n_chunks,)),
            dma((1,)),
            dma((1,)),
            dma((n_chunks,)),
            dma((n_chunks,)),
            dma((2, n_chunks)),
            dma((n_chunks,)),
            dma((3, layers)),
            dma((5,)),
            dma((n_chunks,)),
        ],
        compiler_params=pltpu.CompilerParams(collective_id=0, has_side_effects=True),
    )(
        inputs,
        norm_gain,
        w_value,
        w_gate,
        conv_taps,
        ln_gain,
        ln_bias,
        w_out,
    )


def fits_kernel(n_sp, n_tp, inputs, w_value, conv_taps, w_out):
    rows, dblk = inputs.shape
    width = w_out.shape[2]
    return (
        n_sp == 4 * PAIR
        and n_tp == PAIR * PAIR
        and rows % CHUNK == 0
        and rows // CHUNK >= 4
        and w_value.shape[0] >= 2
        and w_value.shape[1] % LANES == 0
        and w_value.shape[2] % LANES == 0
        and width % LANES == 0
        and dblk == PAIR * width
        and conv_taps.shape[1] - 1 <= HALO
        and HALO * w_value.shape[0] <= CHUNK
        and rows // CHUNK == 4
    )


def shards(inputs, norm_gain, w_value, w_gate, conv_taps, ln_gain, ln_bias, w_out):
    n_sp, n_tp = lax.axis_size("sp"), lax.axis_size("tp")
    args = (inputs, norm_gain, w_value, w_gate, conv_taps, ln_gain, ln_bias, w_out)
    if fits_kernel(n_sp, n_tp, inputs, w_value, conv_taps, w_out):
        return fused_shards(n_sp, n_tp, *args)
    return plain_shards(*args)


def from_behind(block, axis, distance):
    devices = range(lax.axis_size(axis))
    route = [(i - distance, i) for i in devices if i - distance in devices]
    return lax.ppermute(block, axis, route)


def plain_shards(inputs, norm_gain, w_value, w_gate, conv_taps, ln_gain, ln_bias, w_out):
    rows = inputs.shape[0]
    reach = conv_taps.shape[1] - 1
    layers = conv_taps.shape[0]
    channels = conv_taps.shape[2] * lax.axis_size("tp")
    whole_value, whole_gate, whole_out = (
        lax.all_gather(w_value, "sp", axis=1, tiled=True),
        lax.all_gather(w_gate, "sp", axis=1, tiled=True),
        lax.all_gather(w_out, "sp", axis=2, tiled=True),
    )
    stream = inputs
    for layer in range(layers):
        full_rows = lax.all_gather(stream, "tp", axis=1, tiled=True)
        xf = full_rows.astype(jnp.float32)
        meansq = jnp.mean(xf * xf, axis=1, keepdims=True)
        hidden = (xf * lax.rsqrt(meansq + 1e-06) * norm_gain[layer][None, :]).astype(jnp.bfloat16)
        value = jnp.dot(hidden, whole_value[layer], preferred_element_type=jnp.float32)
        gate = jnp.dot(hidden, whole_gate[layer], preferred_element_type=jnp.float32)
        glu = (value * jax.nn.sigmoid(gate)).astype(jnp.bfloat16)
        rim = from_behind(glu[rows - reach :], "sp", 1)
        padded = jnp.concatenate([rim, glu], axis=0)
        count = padded.shape[0] - reach
        filtered = jnp.zeros((count, glu.shape[1]), jnp.float32)
        for tap in range(reach + 1):
            filtered = filtered + conv_taps[layer, tap][None, :] * padded[tap : tap + count].astype(
                jnp.float32
            )
        total_sum, total_sq = lax.psum(
            (jnp.sum(filtered, axis=1), jnp.sum(filtered * filtered, axis=1)), "tp"
        )
        mean_val = (total_sum / channels)[:, None]
        var_val = (total_sq / channels)[:, None] - mean_val * mean_val
        normed = jax.nn.silu(
            (filtered - mean_val) * lax.rsqrt(var_val + 1e-06) * ln_gain[layer][None, :]
            + ln_bias[layer][None, :]
        ).astype(jnp.bfloat16)
        partial_out = jnp.dot(normed, whole_out[layer], preferred_element_type=jnp.float32)
        summed = lax.psum_scatter(
            partial_out.astype(jnp.bfloat16), "tp", scatter_dimension=1, tiled=True
        ).astype(jnp.float32)
        kept = stream.astype(jnp.float32)
        stream = (kept + summed).astype(jnp.bfloat16)
    return stream


def solution(mesh):
    in_specs = (
        P("sp", "tp"),
        P(),
        P(None, "sp", "tp"),
        P(None, "sp", "tp"),
        P(None, None, "tp"),
        P(None, "tp"),
        P(None, "tp"),
        P(None, "tp", "sp"),
    )
    out_specs = P("sp", "tp")
    return jax.shard_map(shards, mesh=mesh, in_specs=in_specs, out_specs=out_specs, check_vma=False)
```

```python
import functools

import jax
import jax.numpy as jnp
from jax import lax
from jax.experimental import pallas as pl
from jax.experimental.pallas import tpu as pltpu
from jax.sharding import PartitionSpec as P

MESH = pl.DeviceIdType.MESH
PAIR = 2
CHUNK = 128
HALO = 32
LANES = 128
V, G, O, UP, OVER, ZOWN, XOWN, BEFORE, SIDE = 0, 1, 2, 3, 4, 5, 6, 7, 8
OWN_X = ((XOWN, V, 1), (XOWN, G, 1))
OWN_Z = ((ZOWN, V, 1), (ZOWN, G, 1))
FIRST, EARLY, RISEN, LAST = 0, 1, 2, 3
LAST_X = ((XOWN, V, 2), (XOWN, G, 2))
LAST_Z = ((ZOWN, V, 2), (ZOWN, G, 2))


def every(kind, later):
    return tuple((kind, j, later) for j in range(4))


END_OPEN = (
    (V, 0, 0), *OWN_Z, (G, 0, 0), (V, 1, 0), (BEFORE, 0, 0), (G, 1, 0), (V, 2, 0), (G, 2, 0), (O, 0, 0),
    (XOWN, V, 1),
)
HEAD_OPEN = (
    (V, 0, 0), *every(UP, 0), *OWN_Z, (G, 0, 0), (V, 1, 0), (BEFORE, 0, 0), (G, 1, 0), (V, 2, 0), (G, 2, 0),
    *every(OVER, 0), *OWN_X,
)
MID_OPEN = (
    (V, 0, 0), (V, 1, 0), (G, 0, 0), (G, 1, 0), (V, 2, 0), (BEFORE, 0, 0), (G, 2, 0),
    (O, 0, 0), (O, 1, 0), (ZOWN, V, 1), (O, 2, 0),
)
NEAR_OPEN = (
    (V, 0, 0), (V, 1, 0), (G, 0, 0), (G, 1, 0), (V, 2, 0), (BEFORE, 0, 0), (G, 2, 0),
    *every(O, 0), *OWN_Z, *OWN_X,
)
SOON_OPEN = (*END_OPEN, (O, 1, 0))
SOON_PLAN = {
    1: ((O, 1, 0, RISEN), (O, 2, 0)), 2: ((O, 3, 0),), 3: ((XOWN, V, 1, RISEN), (XOWN, G, 1)), 4: ((V, 0, 1), *LAST_Z),
    13: ((G, 0, 1, FIRST), (V, 1, 1, FIRST), (V, 2, 1, FIRST)),
    6: ((V, 1, 1, RISEN),), 7: ((V, 2, 1, RISEN), (SIDE, V, 1)), 8: ((G, 0, 1, RISEN), (SIDE, G, 1)),
    9: ((G, 1, 1),), 10: ((G, 2, 1),), 12: ((O, 0, 1),),
}
END_PLAN = {
    1: ((O, 0, 0, RISEN), (O, 1, 0, EARLY)), 2: ((O, 2, 0, EARLY), (O, 1, 0, LAST)),
    3: ((O, 3, 0, EARLY), (XOWN, G, 1)), 14: ((O, 2, 0, LAST),), 4: ((V, 0, 1), *LAST_Z, (O, 3, 0, LAST)),
    13: ((G, 0, 1, FIRST), (V, 1, 1, FIRST), (V, 2, 1, FIRST)),
    6: ((V, 1, 1, RISEN),), 7: ((V, 2, 1, RISEN), (SIDE, V, 1)), 8: ((G, 0, 1, RISEN), (SIDE, G, 1)),
    9: ((G, 1, 1),), 10: ((G, 2, 1),), 12: ((XOWN, V, 2),),
}
HEAD_PLAN = {
    3: every(UP, 1), 5: ((V, 0, 1), *LAST_Z), 6: ((V, 1, 1),), 7: ((V, 2, 1), (SIDE, V, 1)),
    8: ((G, 0, 1), (SIDE, G, 1)), 9: ((G, 1, 1),), 10: ((G, 2, 1), *every(OVER, 1), *LAST_X),
}
MID_PLAN = {
    1: ((O, 3, 0, FIRST), (ZOWN, G, 1), *OWN_X), 2: ((V, 0, 1), (V, 1, 1)), 3: ((V, 2, 1),), 4: ((G, 0, 1), (SIDE, V, 1)),
    5: ((G, 1, 1),), 6: ((G, 2, 1),), 7: ((SIDE, G, 1),),
    9: ((O, 0, 1),), 10: ((O, 1, 1),), 11: ((O, 2, 1),), 12: ((O, 3, 1), (ZOWN, V, 2)),
}
ROOT_PLAN = {
    1: ((V, 0, 1),), 2: ((V, 1, 1),), 3: ((V, 2, 1),), 4: ((G, 0, 1),), 5: ((G, 1, 1), (SIDE, V, 1)),
    6: ((G, 2, 1),), 7: ((SIDE, G, 1), (O, 0, 1), (O, 1, 1)), 8: ((O, 2, 1), (O, 3, 1), *LAST_Z, *LAST_X),
}
NEXT_PLAN = {
    1: ((V, 0, 1),), 2: ((V, 1, 1),), 3: ((V, 2, 1),), 4: ((G, 0, 1), (UP, 0, 1)), 5: ((G, 1, 1), (UP, 1, 1), (SIDE, V, 1)),
    6: ((G, 2, 1), (UP, 2, 1)), 7: ((SIDE, G, 1), (UP, 3, 1)),
    8: (*every(OVER, 1), *LAST_Z, *LAST_X),
}


def fused_kernel(
    n_sp, n_tp, eps,
    x_ref, gain_hbm, wv_ref, wg_ref, taps_hbm, lng_hbm, lnb_hbm, wo_ref,
    out_ref,
    gain_ref, taps_ref, lng_ref, lnb_ref, out_all, wv_all, wg_all, wo_all, xf, hid, glu, filt, stat, nrm,
    w_recv, w_xrecv, w_zsend, w_xsend, o_recv, o_xrecv, o_send, og_send,
    ag_recv, ag_send, before_s, before_r, st_recv, st_send, nr_recv, nr_send,
    in_sem, small_sem, out_sem,
):
    sp = lax.axis_index("sp")
    tp = lax.axis_index("tp")
    layers, depth = wv_ref.shape[0], wv_ref.shape[1]
    rows, dblk = x_ref.shape
    width = wo_ref.shape[2]
    chan = wv_ref.shape[2]
    taps = taps_ref.shape[1]
    features = dblk * n_tp
    channels = chan * n_tp
    n_chunks = rows // CHUNK
    n_out = n_sp // PAIR
    outer, inner = lax.div(sp, PAIR), lax.rem(sp, PAIR)
    x_peer = outer * PAIR + (PAIR - 1 - inner)
    far_half, core = lax.div(tp, PAIR), lax.rem(tp, PAIR)
    partner = far_half * PAIR + (PAIR - 1 - core)
    far = (n_tp // PAIR - 1 - far_half) * PAIR + core
    first_off = HALO - (taps - 1)
    ext = HALO * layers
    halves = chan // LANES

    last = n_out - 1
    upper = lax.div(outer, n_out // 2)
    near_end = outer + upper * (last - 2 * outer)

    def line(j):
        near = j + 1 - (near_end if j == 0 else 0)
        return near + upper * (last - 2 * near)

    slant = sp + 2 * inner - 1
    has_slant = (slant >= 0) & (slant < n_sp)
    barrier = pltpu.get_barrier_semaphore()

    def greet(sp_to, tp_to):
        pl.semaphore_signal(barrier, inc=1, device_id=(sp_to, tp_to), device_id_type=MESH)

    greet(line(0) * PAIR + inner, tp)
    greet(x_peer, tp)
    for step in range(1, n_tp):
        greet(sp, lax.rem(tp + step, n_tp))

    @pl.when(near_end == 1)
    def _():
        greet(line(1) * PAIR + inner, tp)

    @pl.when(has_slant)
    def _():
        greet(slant, tp)

    def own_rows(s):
        return pl.ds(pl.multiple_of(s * depth, depth), depth)

    def o_slot(l, x, b):
        return wo_all.at[l, x, pl.ds(pl.multiple_of(b * chan, chan), chan), :]

    def load_weight(m, l):
        src, dst = ((wv_ref, wv_all), (wg_ref, wg_all))[m]
        return pltpu.make_async_copy(src.at[l], dst.at[l, own_rows(sp), :], in_sem.at[0 if l == 0 else 1])

    def load_out(l):
        return pltpu.make_async_copy(wo_ref.at[l], o_slot(l, inner, tp), in_sem.at[2])

    def load_rows():
        return pltpu.make_async_copy(x_ref, xf.at[tp, pl.ds(ext, rows), :], small_sem.at[4])

    smalls = [
        pltpu.make_async_copy(src, dst, small_sem.at[i])
        for i, (src, dst) in enumerate(
            ((gain_hbm, gain_ref), (taps_hbm, taps_ref), (lng_hbm, lng_ref), (lnb_hbm, lnb_ref)))
    ]
    for m in range(PAIR):
        load_weight(m, 0).start()
    load_rows().start()

    @pl.when(outer == tp)
    def _():
        for l in range(layers):
            load_out(l).start()

    for l in range(1, layers):
        for m in range(PAIR):
            load_weight(m, l).start()
    for small in smalls:
        small.start()

    glu[:, 0:HALO, :] = jnp.zeros((halves, HALO, LANES), jnp.float32)

    @pl.when(sp == 0)
    def _():
        xf[tp, 0:ext, :] = jnp.zeros((ext, dblk), jnp.bfloat16)


    def loaded(block, k):
        pltpu.make_async_copy(block, block, in_sem.at[k]).wait()

    loaded(wv_all.at[0, pl.ds(0, PAIR * depth), :], 0)
    pl.semaphore_wait(barrier, 2 + n_tp - 1 + near_end + has_slant.astype(jnp.int32))

    def parts(c):
        own = (ext + c * CHUNK, CHUNK)
        return ((0, ext), own) if c == 0 else (own,)

    def chunk_rows(c, skip):
        return pl.ds(ext + c * CHUNK, CHUNK) if c else pl.ds(skip * HALO, ext - skip * HALO + CHUNK)

    def by_layer(c, l, f):
        if c or isinstance(l, int):
            f(0 if c else l)
        else:
            for k in range(layers):
                pl.when(l == k)(functools.partial(f, k))

    def stat_rows(c):
        return pl.ds(0, 8 * len(parts(c)))

    def remote(src, dst, send, recv, sp_to, tp_to):
        return pltpu.make_async_remote_copy(
            src_ref=src, dst_ref=dst, send_sem=send, recv_sem=recv,
            device_id=(sp_to, tp_to), device_id_type=MESH,
        )

    def w_slot(m, l, s):
        return (wv_all, wg_all)[m].at[l, own_rows(s), :]

    def z_copy(m, l, j):
        to = line(j) * PAIR + inner
        return remote(w_slot(m, l, sp), w_slot(m, l, sp), w_zsend.at[m], w_recv.at[l, m, outer], to, tp)

    def z_arrival(m, l, j):
        s = line(j) * PAIR + inner
        return remote(w_slot(m, l, s), w_slot(m, l, s), w_zsend.at[m], w_recv.at[l, m, line(j)], s, tp)

    def z_forward(m, l, j):
        s = line(j) * PAIR + inner
        to = line(1 if j == 0 else 0) * PAIR + inner
        slot = w_slot(m, l, s)
        return remote(slot, slot, w_zsend.at[m], w_recv.at[l, m, line(j)], to, tp)

    def x_own(m, l):
        return remote(w_slot(m, l, sp), w_slot(m, l, sp), w_xsend.at[m], w_xrecv.at[l, m, 0], x_peer, tp)

    def x_copy(m, l, j):
        s = line(j) * PAIR + inner
        slot = w_slot(m, l, s)
        return remote(slot, slot, w_xsend.at[m], w_xrecv.at[l, m, 1], x_peer, tp)

    def x_arrival(m, l):
        slot = w_slot(m, l, x_peer)
        return remote(slot, slot, w_xsend.at[m], w_xrecv.at[l, m, 0], x_peer, tp)

    def x_arrivals(m, l):
        block = (wv_all, wg_all)[m].at[l, pl.ds(0, last * depth), :]
        return remote(block, block, w_xsend.at[m], w_xrecv.at[l, m, 1], x_peer, tp)

    def side_copy(m, l):
        to = line(0) * PAIR + inner
        slot = w_slot(m, l, x_peer)
        return remote(slot, slot, w_xsend.at[m], w_xrecv.at[l, m, 1], to, tp)

    def z_own(m, l):
        z_copy(m, l, 0).start()

        @pl.when(near_end == 1)
        def _():
            z_copy(m, l, 1).start()

    def relay_piece(m, l, j, side):
        z_arrival(m, l, j).wait_recv()

        @pl.when(near_end == 1)
        def _():
            z_forward(m, l, j).start()

        if j or not side:
            x_copy(m, l, j).start()
        elif m == V:
            @pl.when(jnp.logical_not(by_side(m, l)))
            def _():
                x_copy(m, l, j).start()

    def by_side(m, l):
        return l > 0 if m == G else (l > 0) & ((l < layers - 1) | (upper == far_half))

    def relay_side(m, l):
        @pl.when(by_side(m, l))
        def _():
            x_arrival(m, l).wait_recv()
            side_copy(m, l).start()

    def w_ready(m, l):
        @pl.when(jnp.logical_not(by_side(m, l)))
        def _():
            x_arrival(m, l).wait_recv()

        x_arrivals(m, l).wait_recv()

    def o_gather(l):
        return remote(wo_ref.at[l], o_slot(l, inner, tp), og_send.at[0], o_recv.at[l, tp], sp, outer)

    def o_hop(l, j, way, to):
        b = lax.rem(tp + j, n_tp)
        slot = o_slot(l, inner, b)
        return remote(slot, slot, o_send.at[way], o_xrecv.at[l] if way == 2 else o_recv.at[l, b], to, tp)

    def o_arrival(l, b):
        slot = o_slot(l, inner, b)
        return remote(slot, slot, o_send.at[0], o_recv.at[l, b], x_peer, tp)

    goes_up = (outer >= tp) & (outer < last)
    goes_down = (outer <= tp) & (outer > 0)

    def send_o(l):
        @pl.when(outer != tp)
        def _():
            o_gather(l).start()

    def o_arrived(l, j):
        if j == 0:
            @pl.when(outer != tp)
            def _():
                o_arrival(l, tp).wait_recv()
        else:
            o_arrival(l, lax.rem(tp + j, n_tp)).wait_recv()

    def o_along(l, j):
        @pl.when(goes_up)
        def _():
            o_hop(l, j, 0, sp + PAIR).start()

        @pl.when(goes_down)
        def _():
            o_hop(l, j, 1, sp - PAIR).start()

    def relay_o(l, j, kind):
        if kind != OVER:
            o_arrived(l, j)
            o_along(l, j)
        if kind != UP:
            o_hop(l, j, 2, x_peer).start()

    def o_ready(l):
        block = wo_all.at[l, 0]
        remote(block, block, o_send.at[2], o_xrecv.at[l], x_peer, tp).wait_recv()

    def ag_far(c, l):
        r = chunk_rows(c, l)
        return remote(xf.at[tp, r, :], xf.at[tp, r, :], ag_send.at[c], ag_recv.at[0, c], sp, far)

    def ag_partner(c, l):
        r = chunk_rows(c, l)
        return remote(xf.at[tp, r, :], xf.at[tp, r, :], ag_send.at[c], ag_recv.at[1, c], sp, partner)

    def ag_forward(c, l):
        r = chunk_rows(c, l)
        return remote(xf.at[far, r, :], xf.at[far, r, :], ag_send.at[c], ag_recv.at[1, c], sp, partner)

    def nr_far(c, l):
        r = chunk_rows(c, l + 1)
        return remote(nrm.at[tp, r, :], nrm.at[tp, r, :], nr_send.at[c], nr_recv.at[0, c], sp, far)

    def nr_partner(c, l):
        r = chunk_rows(c, l + 1)
        return remote(nrm.at[tp, r, :], nrm.at[tp, r, :], nr_send.at[c], nr_recv.at[1, c], sp, partner)

    def nr_forward(c, l):
        r = chunk_rows(c, l + 1)
        return remote(nrm.at[far, r, :], nrm.at[far, r, :], nr_send.at[c], nr_recv.at[1, c], sp, partner)

    def stat_copy(l, c, step):
        to = lax.rem(tp + step, n_tp)
        return remote(stat.at[l, c, tp, stat_rows(c), :], stat.at[l, c, tp, stat_rows(c), :], st_send.at[c], st_recv.at[c], sp, to)

    def stats(l, c):
        block = stat.at[l, c, pl.ds(0, n_tp - 1), stat_rows(c), :]
        return remote(block, block, st_send.at[c], st_recv.at[c], sp, far)

    def before_copy():
        to = lax.rem(sp + 1, n_sp)
        return remote(x_ref.at[pl.ds(rows - ext, ext), :], xf.at[tp, pl.ds(0, ext), :], before_s.at[0], before_r.at[0], to, tp)

    def do_pass(l, c):
        def go(k):
            ag_far(c, k).wait_recv()
            ag_forward(c, k).start()

        by_layer(c, l, go)

    def ag_start(l, c):
        def go(k):
            ag_far(c, k).start()
            ag_partner(c, k).start()

        by_layer(c, l, go)

    def ag_sent(l, c):
        def go(k):
            block = xf.at[pl.ds(0, 3), chunk_rows(c, k), :]
            remote(block, block, ag_send.at[c], ag_recv.at[1, c], sp, far).wait_send()

        by_layer(c, l, go)

    def ag_wait(l, c):
        def go(k):
            block = xf.at[pl.ds(0, PAIR), chunk_rows(c, k), :]
            remote(block, block, ag_send.at[c], ag_recv.at[1, c], sp, partner).wait_recv()

        by_layer(c, l, go)

    def nr_start(l, c):
        def go(k):
            nr_far(c, k).start()
            nr_partner(c, k).start()

        by_layer(c, l, go)

    def nr_sent(l, c):
        def go(k):
            block = nrm.at[pl.ds(0, 3), chunk_rows(c, k + 1), :]
            remote(block, block, nr_send.at[c], nr_recv.at[1, c], sp, far).wait_send()

        by_layer(c, l, go)

    def nr_wait(l, c):
        def go(k):
            block = nrm.at[pl.ds(0, PAIR), chunk_rows(c, k + 1), :]
            remote(block, block, nr_send.at[c], nr_recv.at[1, c], sp, partner).wait_recv()

        by_layer(c, l, go)

    def do_glu(l, cs):
        for c in cs:
            ag_wait(l, c)

        def glu_part(start, size):
            r = slice(start, start + size)
            blocks = [xf[b, r, :].astype(jnp.float32) for b in range(n_tp)]
            total = sum(jnp.sum(b * b, axis=1, keepdims=True) for b in blocks)
            scale = lax.rsqrt(total / features + eps)
            for b in range(n_tp):
                cols = slice(b * dblk, (b + 1) * dblk)
                hid[0:size, cols] = (
                    xf[b, r, :].astype(jnp.float32) * scale * gain_ref[pl.ds(l, 1), cols]).astype(jnp.bfloat16)
            h = hid[0:size, :]
            value = jnp.dot(h, wv_all[l], preferred_element_type=jnp.float32)
            gate = jnp.dot(h, wg_all[l], preferred_element_type=jnp.float32)
            g = (value * jax.nn.sigmoid(gate)).astype(jnp.bfloat16).astype(jnp.float32)
            if start < ext:
                row = lax.broadcasted_iota(jnp.int32, g.shape, 0)
                g = jnp.where((row >= ext - start) | (sp > 0), g, 0.0)
            for k in range(halves):
                glu[k, HALO + start:HALO + start + size, :] = g[:, k * LANES:(k + 1) * LANES]

        start, size = ext + cs[0] * CHUNK, len(cs) * CHUNK
        if cs[0]:
            glu_part(start, size)
        else:
            pl.when(l < layers - 1)(functools.partial(glu_part, 0, start + size))
            pl.when(l == layers - 1)(functools.partial(glu_part, ext - HALO, HALO + size))

    def do_conv(l, c):
        def conv_part(i, start, size):
            sums = jnp.zeros((size, 1), jnp.float32)
            squares = jnp.zeros((size, 1), jnp.float32)
            for k in range(halves):
                acc = jnp.zeros((size, LANES), jnp.float32)
                for tap in range(taps):
                    acc = acc + taps_ref[l, tap:tap + 1, k * LANES:(k + 1) * LANES] * glu[
                        k, start + first_off + tap:start + first_off + tap + size, :]
                filt[start:start + size, k * LANES:(k + 1) * LANES] = acc
                sums = sums + jnp.sum(acc, axis=1, keepdims=True)
                squares = squares + jnp.sum(acc * acc, axis=1, keepdims=True)
            lane = lax.broadcasted_iota(jnp.int32, (size, LANES), 1)
            both = jnp.where(lane == 0, sums, squares)
            if size < CHUNK:
                both = jnp.concatenate([both, jnp.zeros((CHUNK - size, LANES), jnp.float32)], axis=0)
            stat[l, c, tp, 8 * i:8 * i + 8, :] = jnp.transpose(both)[0:8, :]

        for i, (start, size) in enumerate(parts(c)):
            if start < ext:
                pl.when(l < layers - 1)(functools.partial(conv_part, i, start, size))
            else:
                conv_part(i, start, size)
        for step in range(1, n_tp):
            stat_copy(l, c, step).start()

    def do_norm(l, c):
        stats(l, c).wait_recv()

        def norm_part(i, start, size):
            r = slice(start, start + size)
            tot = stat[l, c, 0, 8 * i:8 * i + 8, :]
            for b in range(1, n_tp):
                tot = tot + stat[l, c, b, 8 * i:8 * i + 8, :]
            tot = jnp.transpose(jnp.concatenate([tot, jnp.zeros((LANES - 8, CHUNK), jnp.float32)], axis=0))
            mean = tot[0:size, 0:1] / channels
            var = tot[0:size, 1:2] / channels - mean * mean
            pre = (filt[r, :] - mean) * lax.rsqrt(var + eps) * lng_ref[pl.ds(l, 1), :] + lnb_ref[pl.ds(l, 1), :]
            nrm[tp, r, :] = jax.nn.silu(pre).astype(jnp.bfloat16)

        for i, (start, size) in enumerate(parts(c)):
            pl.when((start >= ext) | (l < layers - 1))(functools.partial(norm_part, i, start, size))
        ag_sent(l, c)
        stats(l, c).wait_send()
        nr_start(l, c)

    def do_hand(l, c):
        def go(k):
            nr_far(c, k).wait_recv()
            nr_forward(c, k).start()

        by_layer(c, l, go)

    def store_rows(c):
        r = pl.ds(c * CHUNK, CHUNK)
        return pltpu.make_async_copy(out_all.at[r, :], out_ref.at[r, :], out_sem.at[0])

    def do_half(l, c, q, final):
        for start, size in parts(c):
            if final and start < ext:
                continue
            r = slice(start, start + size)
            cols = pl.ds(pl.multiple_of(q * width, width), width)
            full = jnp.concatenate([nrm[b, r, :] for b in range(n_tp)], axis=1)
            branch = jnp.dot(full, wo_all[l, q], preferred_element_type=jnp.float32)
            new = (xf[tp, r, cols].astype(jnp.float32) + branch).astype(jnp.bfloat16)
            if final:
                out_all[start - ext:start - ext + size, cols] = new
            else:
                xf[tp, r, cols] = new

    def do_near(l, c, final):
        nr_wait(l, c)
        do_half(l, c, inner, final)

    def do_rest(l, c):
        do_half(l, c, PAIR - 1 - inner, False)
        ag_start(l + 1, c)
        nr_sent(l, c)

    by_head = near_end * (outer - tp) * (outer - tp) * (1 - (far_half - core) * (far_half - core)) == 1
    is_root = (near_end == 1) & (outer == tp)
    is_mid = (near_end == 1) & (outer != tp) & jnp.logical_not(by_head)
    is_head = (near_end == 0) & (outer == tp)
    is_soon = (near_end == 0) & ((outer - tp) * (outer - tp) == 1)
    is_end = (near_end == 0) & ((outer - tp) * (outer - tp) > 1)

    roles = (
        (is_end, END_OPEN, END_PLAN), (is_soon, SOON_OPEN, SOON_PLAN), (is_head, HEAD_OPEN, HEAD_PLAN),
        (is_mid, MID_OPEN, MID_PLAN), (is_root, NEAR_OPEN, ROOT_PLAN), (by_head, NEAR_OPEN, NEXT_PLAN),
    )

    def act(kind, j, l, side):
        if kind == BEFORE:
            @pl.when(sp > 0)
            def _():
                before_copy().wait_recv()

            ag_start(0, 0)
        elif kind == SIDE:
            relay_side(j, l)
        elif kind == ZOWN:
            z_own(j, l)
        elif kind == XOWN:
            x_own(j, l).start()
        elif kind >= O:
            relay_o(l, j, kind)
        else:
            relay_piece(kind, l, j, side)

    for m in (V, G):
        z_own(m, 0)
        x_own(m, 0).start()
    @pl.when(sp < n_sp - 1)
    def _():
        before_copy().start()

    send_o(0)
    load_rows().wait()
    for c in range(1, n_chunks):
        ag_start(0, c)
    loaded(wv_all.at[pl.ds(1, layers - 1), pl.ds(0, PAIR * depth), :], 1)

    @pl.when(outer == tp)
    def _():
        loaded(wo_all.at[:, 0, pl.ds(0, chan), :], 2)

    for small in smalls:
        small.wait()
    send_o(1)
    for role, order, _ in roles:
        @pl.when(role)
        def _():
            for kind, j, later in order:
                act(kind, j, later, False)

    for c in range(n_chunks):
        do_pass(0, c)
    w_ready(V, 0)
    w_ready(G, 0)

    def layer_body(l, carry):
        more = l < layers - 1

        def ahead(f):
            pl.when(more)(f)

        def slot(n):
            for role, _, plan in roles:
                for kind, j, later, *turn in plan.get(n, ()):
                    when = (role & (l + later < layers)) if later else role
                    for t in turn:
                        when = when & (l == 0, l < layers - 1, l > 0, l == layers - 1)[t]

                    @pl.when(when)
                    def _():
                        act(kind, j, l + later, True)

        def pass_next(c):
            ahead(lambda: do_pass(l + 1, c))

        do_glu(l, (0,))
        do_conv(l, 0)
        slot(1)
        do_glu(l, (1,))
        do_conv(l, 1)
        do_glu(l, (2, 3))
        do_conv(l, 2)
        slot(2)
        do_norm(l, 0)
        do_conv(l, 3)
        do_norm(l, 1)
        slot(3)
        do_norm(l, 2)
        slot(14)
        do_norm(l, 3)
        slot(4)
        @pl.when(more)
        def _():
            do_hand(l, 0)
            slot(5)
            do_hand(l, 1)
            slot(13)
            o_ready(l)
            do_near(l, 0, False)
            do_rest(l, 0)
            do_hand(l, 2)
            do_near(l, 1, False)
            do_rest(l, 1)
            slot(6)
            do_hand(l, 3)
            do_near(l, 2, False)
            do_rest(l, 2)
            slot(7)
            do_near(l, 3, False)
            do_rest(l, 3)

        @pl.when(l == layers - 1)
        def _():
            do_hand(l, 0)
            do_hand(l, 1)
            do_near(l, 0, True)
            do_hand(l, 2)
            do_near(l, 1, True)
            do_hand(l, 3)
            do_near(l, 2, True)
            do_near(l, 3, True)
            o_ready(l)
            for c in range(0, n_chunks, PAIR):
                r = slice(c * CHUNK, (c + PAIR) * CHUNK)
                q = PAIR - 1 - inner
                cols = pl.ds(pl.multiple_of(q * width, width), width)
                x_rows = slice(ext + c * CHUNK, ext + (c + PAIR) * CHUNK)
                full = jnp.concatenate([nrm[b, x_rows, :] for b in range(n_tp)], axis=1)
                branch = jnp.dot(full, wo_all[l, q], preferred_element_type=jnp.float32)
                out_all[r, cols] = (xf[tp, x_rows, cols].astype(jnp.float32) + branch).astype(jnp.bfloat16)
                for k in range(c, c + PAIR):
                    store_rows(k).start()
            for c in range(n_chunks):
                nr_sent(l, c)

        @pl.when(l < layers - 2)
        def _():
            send_o(l + 2)

        slot(8)
        pass_next(0)
        slot(9)
        pass_next(1)
        slot(10)
        pass_next(2)
        slot(11)
        pass_next(3)
        slot(12)

        @pl.when(more)
        def _():
            w_ready(V, l + 1)
            w_ready(G, l + 1)

        return carry

    lax.fori_loop(0, layers, layer_body, 0)

    def sent(block, sem):
        remote(block, block, sem, before_r.at[0], x_peer, tp).wait_send()

    for m in range(PAIR):
        whole = (wv_all, wg_all)[m]
        sent(whole.at[:, pl.ds(0, n_out * depth), :], w_xsend.at[m])

        @pl.when(near_end == 0)
        def _():
            sent(whole.at[:, pl.ds(0, depth), :], w_zsend.at[m])

        @pl.when(near_end == 1)
        def _():
            sent(whole.at[:, pl.ds(0, (PAIR + last) * depth), :], w_zsend.at[m])

    @pl.when(outer != tp)
    def _():
        sent(wo_all.at[:, 0, pl.ds(0, chan), :], og_send.at[0])

    @pl.when(goes_up)
    def _():
        sent(wo_all.at[:, 0], o_send.at[0])

    @pl.when(goes_down)
    def _():
        sent(wo_all.at[:, 0], o_send.at[1])

    sent(wo_all.at[:, 0], o_send.at[2])

    @pl.when(sp < n_sp - 1)
    def _():
        before_copy().wait_send()

    pltpu.make_async_copy(out_all, out_ref, out_sem.at[0]).wait()


def fused_shards(n_sp, n_tp, inputs, norm_gain, w_value, w_gate, conv_taps, ln_gain, ln_bias, w_out):
    layers, depth, chan = w_value.shape
    rows, dblk = inputs.shape
    width = w_out.shape[2]
    n_chunks = rows // CHUNK
    features = dblk * n_tp
    ext = HALO * layers
    bf16, f32 = jnp.bfloat16, jnp.float32
    dma = pltpu.SemaphoreType.DMA
    place = pl.BlockSpec(memory_space=pl.ANY)
    return pl.pallas_call(
        functools.partial(fused_kernel, n_sp, n_tp, 1e-06),
        out_shape=jax.ShapeDtypeStruct((rows, dblk), bf16),
        in_specs=[place] * 8,
        out_specs=place,
        scratch_shapes=[
            pltpu.VMEM(norm_gain.shape, f32),
            pltpu.VMEM(conv_taps.shape, f32),
            pltpu.VMEM(ln_gain.shape, f32),
            pltpu.VMEM(ln_bias.shape, f32),
            pltpu.VMEM((rows, dblk), bf16),
            pltpu.VMEM((layers, n_sp * depth, chan), bf16),
            pltpu.VMEM((layers, n_sp * depth, chan), bf16),
            pltpu.VMEM((layers, PAIR, n_tp * chan, width), bf16),
            pltpu.VMEM((n_tp, ext + rows, dblk), bf16),
            pltpu.VMEM((ext + PAIR * CHUNK, features), bf16),
            pltpu.VMEM((chan // LANES, HALO + ext + rows, LANES), f32),
            pltpu.VMEM((ext + rows, chan), f32),
            pltpu.VMEM((layers, n_chunks, n_tp, 16, CHUNK), f32),
            pltpu.VMEM((n_tp, ext + rows, chan), bf16),
            dma((layers, PAIR, n_sp // PAIR)),
            dma((layers, PAIR, 2)),
            dma((PAIR,)),
            dma((PAIR,)),
            dma((layers, n_tp)),
            dma((layers,)),
            dma((3,)),
            dma((1,)),
            dma((2, n_chunks)),
            dma((n_chunks,)),
            dma((1,)),
            dma((1,)),
            dma((n_chunks,)),
            dma((n_chunks,)),
            dma((2, n_chunks)),
            dma((n_chunks,)),
            dma((3,)),
            dma((5,)),
            dma((1,)),
        ],
        compiler_params=pltpu.CompilerParams(collective_id=0, has_side_effects=True),
    )(
        inputs,
        norm_gain,
        w_value,
        w_gate,
        conv_taps,
        ln_gain,
        ln_bias,
        w_out,
    )


def fits_kernel(n_sp, n_tp, inputs, w_value, conv_taps, w_out):
    rows, dblk = inputs.shape
    width = w_out.shape[2]
    return (
        n_sp == 4 * PAIR
        and n_tp == PAIR * PAIR
        and rows % CHUNK == 0
        and rows // CHUNK >= 4
        and w_value.shape[0] >= 2
        and w_value.shape[1] % LANES == 0
        and w_value.shape[2] % LANES == 0
        and width % LANES == 0
        and dblk == PAIR * width
        and conv_taps.shape[1] - 1 <= HALO
        and HALO * w_value.shape[0] <= CHUNK
        and rows // CHUNK == 4
    )


def shards(inputs, norm_gain, w_value, w_gate, conv_taps, ln_gain, ln_bias, w_out):
    n_sp, n_tp = lax.axis_size("sp"), lax.axis_size("tp")
    args = (inputs, norm_gain, w_value, w_gate, conv_taps, ln_gain, ln_bias, w_out)
    if fits_kernel(n_sp, n_tp, inputs, w_value, conv_taps, w_out):
        return fused_shards(n_sp, n_tp, *args)
    return plain_shards(*args)


def from_behind(block, axis, distance):
    devices = range(lax.axis_size(axis))
    route = [(i - distance, i) for i in devices if i - distance in devices]
    return lax.ppermute(block, axis, route)


def plain_shards(inputs, norm_gain, w_value, w_gate, conv_taps, ln_gain, ln_bias, w_out):
    rows = inputs.shape[0]
    reach = conv_taps.shape[1] - 1
    layers = conv_taps.shape[0]
    channels = conv_taps.shape[2] * lax.axis_size("tp")
    whole_value, whole_gate, whole_out = (
        lax.all_gather(w_value, "sp", axis=1, tiled=True),
        lax.all_gather(w_gate, "sp", axis=1, tiled=True),
        lax.all_gather(w_out, "sp", axis=2, tiled=True),
    )
    stream = inputs
    for layer in range(layers):
        full_rows = lax.all_gather(stream, "tp", axis=1, tiled=True)
        xf = full_rows.astype(jnp.float32)
        meansq = jnp.mean(xf * xf, axis=1, keepdims=True)
        hidden = (xf * lax.rsqrt(meansq + 1e-06) * norm_gain[layer][None, :]).astype(jnp.bfloat16)
        value = jnp.dot(hidden, whole_value[layer], preferred_element_type=jnp.float32)
        gate = jnp.dot(hidden, whole_gate[layer], preferred_element_type=jnp.float32)
        glu = (value * jax.nn.sigmoid(gate)).astype(jnp.bfloat16)
        rim = from_behind(glu[rows - reach :], "sp", 1)
        padded = jnp.concatenate([rim, glu], axis=0)
        count = padded.shape[0] - reach
        filtered = jnp.zeros((count, glu.shape[1]), jnp.float32)
        for tap in range(reach + 1):
            filtered = filtered + conv_taps[layer, tap][None, :] * padded[tap : tap + count].astype(
                jnp.float32
            )
        total_sum, total_sq = lax.psum(
            (jnp.sum(filtered, axis=1), jnp.sum(filtered * filtered, axis=1)), "tp"
        )
        mean_val = (total_sum / channels)[:, None]
        var_val = (total_sq / channels)[:, None] - mean_val * mean_val
        normed = jax.nn.silu(
            (filtered - mean_val) * lax.rsqrt(var_val + 1e-06) * ln_gain[layer][None, :]
            + ln_bias[layer][None, :]
        ).astype(jnp.bfloat16)
        partial_out = jnp.dot(normed, whole_out[layer], preferred_element_type=jnp.float32)
        summed = lax.psum_scatter(
            partial_out.astype(jnp.bfloat16), "tp", scatter_dimension=1, tiled=True
        ).astype(jnp.float32)
        kept = stream.astype(jnp.float32)
        stream = (kept + summed).astype(jnp.bfloat16)
    return stream


def solution(mesh):
    in_specs = (
        P("sp", "tp"),
        P(),
        P(None, "sp", "tp"),
        P(None, "sp", "tp"),
        P(None, None, "tp"),
        P(None, "tp"),
        P(None, "tp"),
        P(None, "tp", "sp"),
    )
    out_specs = P("sp", "tp")
    return jax.shard_map(shards, mesh=mesh, in_specs=in_specs, out_specs=out_specs, check_vma=False)
```
